32 devices in a mesh: ep: 8 (over z, y), tp: 4 (over x, core).
Axes of the slice: x: 2, y: 2, z: 4, core: 2. Of those that a mesh axis runs over, the one named last changes fastest.
Arguments:
- query_rows: bfloat16 [3072, 1024], P('ep', 'tp'), may hold values from -6 to 6
- key_rows: bfloat16 [3072, 512], P('ep', 'tp'), may hold values from -6 to 6
- value_rows: bfloat16 [3072, 512], P('ep', 'tp'), may hold values from -6 to 6
- break_bias: bfloat16 [3072, 16], P('ep', 'tp'), may hold values from -14 to 0
- mixer_weight: bfloat16 [1024, 2048], P('tp'), may hold values from -0.1875 to 0.1875
- mixer_gain: bfloat16 [2048], replicated, may hold values from 0.099609375 to 1.8984375
- expert_input: bfloat16 [4096, 2048], P(('ep', 'tp')), may hold values from -6 to 6
- expert_gain: bfloat16 [2048], replicated, may hold values from 0.099609375 to 1.8984375
- route_ids: int32 [4096, 2], P('ep'), may hold values from 0 to 15, all different within a row; in each aligned block of 128 rows (0 to 127, 128 to 255, ...) at most 32 rows name the same one
- route_weights: float32 [4096, 2], P(('ep', 'tp')), may hold values from 0.2 to 2
- expert_gate: bfloat16 [16, 2048, 2048], P('ep', None, 'tp'), may hold values from -0.125 to 0.125
- expert_up: bfloat16 [16, 2048, 2048], P('ep', None, 'tp'), may hold values from -0.125 to 0.125
- expert_down: bfloat16 [16, 2048, 2048], P('ep', 'tp'), may hold values from -0.125 to 0.125
- shared_gate: bfloat16 [2048, 512], replicated, may hold values from -0.125 to 0.125
- shared_up: bfloat16 [2048, 512], replicated, may hold values from -0.125 to 0.125
- shared_down: bfloat16 [512, 2048], replicated, may hold values from -0.25 to 0.25
Outputs:
- mixer_out: bfloat16 [3072, 2048], P(('ep', 'tp'))
- expert_out: bfloat16 [4096, 2048], P(('ep', 'tp'))
The draws below stay inside these ranges and needn't reach their ends.
Inputs may be any that keep to these rules, and one draw needn't show every extreme that they name: `route_ids`: each row names 2 different experts. Within the rows of one device no expert is named more than 32 times, and in every draw some expert is named exactly 32 times within the rows of some device.
All inputs are finite; a program needn't handle non-finite values.
Results may differ from the reference program's by a relative error of at most 0.012.
Values may be sent and summed in bfloat16 or wider, within the bound.
A program may use at most 192 MiB of HBM per device.

```python
import math
import jax
import jax.numpy as jnp
import numpy as np
from jax import lax

D = 2048
DH = 64
HEADS = 16
KV_HEADS = 8
FF_E = 2048
SHARED_FF = 512
TOPK = 2
SEQS = 1
TOK_A_DEV = 384
TOK_B_DEV = 128
EXPERTS = 16
CAP = 32
ATTENTION_TOKENS = 3072
SEQUENCE_LENGTH = 3072
TOKENS_B = 4096
N_EP = 8
N_TP = 4


def draw_break_bias(key, part):
    head_random_key, perturb_random_key, block_random_key, spike_random_key, noise_random_key = jax.random.split(jax.random.fold_in(key, 17), 5)
    slow_share = 0.5
    slow = jax.random.uniform(head_random_key, (HEADS,)) < slow_share
    base = jnp.where(slow, jnp.log(0.8 / SEQUENCE_LENGTH), jnp.log(1.0 / 40.0))
    base = base + 0.3 * jax.random.normal(perturb_random_key, (HEADS,))
    blocks = jax.random.uniform(block_random_key, (ATTENTION_TOKENS // TOK_A_DEV, 1), minval=-1.05, maxval=1.05)
    magnitude_level = jnp.repeat(blocks, TOK_A_DEV, axis=0) + base[None, :]
    spike_batch = jax.random.uniform(spike_random_key, (ATTENTION_TOKENS, 1)) < 4.0 / SEQUENCE_LENGTH
    magnitude_level = jnp.where(spike_batch, -0.8, magnitude_level)
    magnitude_level = magnitude_level + 0.3 * jax.random.normal(noise_random_key, (ATTENTION_TOKENS, HEADS))
    return jnp.clip(magnitude_level, -14.0, 0.0).astype(jnp.bfloat16)


def block_scale(key, dims, cuts, least, high):
    def one(position, shards_of):
        heights = jax.random.uniform(jax.random.fold_in(jax.random.fold_in(key, 6), position), (shards_of,), jnp.float32, least / len(cuts), high / len(cuts))
        return jnp.repeat(jnp.exp(heights), dims[position] // shards_of).reshape((-1,) + (1,) * (len(dims) - position - 1))

    factor_of = one(*cuts[0])
    for cut in cuts[1:]:
        factor_of = factor_of * one(*cut)
    return factor_of


def deal_out(own_key, own, number, rows, number_of, top, most, skew):
    ranking = jax.random.permutation(own_key, number_of)
    packed, common = portions_of(number_of, rows * top, most, skew, True), portions_of(number_of, rows * top, most, skew, False)
    places = jnp.arange(number_of)

    def named(sizes, turn):
        used = int((sizes > 0).sum())
        fixed = max(1, used // 4)
        passed = fixed + (places - fixed + turn * (used - fixed)) % max(1, number_of - fixed)
        return jnp.zeros((number_of,), jnp.int32).at[ranking[jnp.where(places < fixed, places, passed)]].set(jnp.asarray(sizes, jnp.int32))

    sizes = jnp.where(number % 4 == 0, named(packed, number // 4), named(common, number - number // 4 - 1))
    mixed = jax.random.permutation(jax.random.fold_in(own, 3), number_of)
    giver, sink = mixed[0:number_of // 2 * 2:2], mixed[1:number_of // 2 * 2:2]
    slack = jnp.minimum(sizes[giver] - 1, most - sizes[sink]) // 2
    slack = jnp.where((giver == ranking[0]) | (sink == ranking[0]) | (sizes[sink] == 0), 0, jnp.maximum(slack, 0))
    passed = jax.random.randint(jax.random.fold_in(own, 4), (number_of // 2,), 0, 1 << 20) % (slack + 1)
    sizes = sizes.at[giver].add(-passed).at[sink].add(passed)
    labels = jnp.searchsorted(jnp.cumsum(sizes), jnp.arange(rows * top), side="right").astype(jnp.int32)
    listing = labels.reshape(top, rows).T
    listing = listing[jax.random.permutation(jax.random.fold_in(own, 1), rows)]
    turn = jax.random.randint(jax.random.fold_in(own, 2), (rows, 1), 0, top)
    return jnp.take_along_axis(listing, (jnp.arange(top)[None, :] + turn) % top, axis=1)


def portions_of(number_of, total, most, skew, full):
    loads = [(1 << 20) // math.isqrt(rank ** skew) + 1 for rank in range(1, number_of + 1)]
    largest = most if full else min(most, max(-(-total // number_of), total * loads[0] // sum(loads)))
    least = 1 if total - largest >= number_of - 1 else 0
    holding, rest = [largest] + [least] * (number_of - 1), total - largest - least * (number_of - 1)
    while rest > 0:
        free = [i for i in range(1, number_of) if holding[i] < largest] or [i for i in range(1, number_of) if holding[i] < most]
        pool, remaining = sum([loads[i] for i in free]), rest
        for i in free:
            addition = min(most - holding[i], max(1, remaining * loads[i] // pool), rest)
            holding[i] = holding[i] + addition
            rest = rest - addition
    return np.array(holding)


def gaussian(stream_key, extent, width, limit, cuts=(), kind=jnp.bfloat16):
    level = block_scale(stream_key, extent, cuts, -0.22, 0.18) if cuts else 1.0
    values = jax.random.normal(stream_key, extent, jnp.float32) * width * level
    return jnp.minimum(jnp.maximum(values, -limit), limit).astype(kind)


def setup_inputs(seed: int = 0) -> dict:
    arg_keys = jax.random.split(jax.random.key(seed), 17)
    query_rows = gaussian(arg_keys[0], (ATTENTION_TOKENS, HEADS * DH), 1.0, 6.0, ((0, 8), (1, 4)))
    key_rows = gaussian(arg_keys[1], (ATTENTION_TOKENS, KV_HEADS * DH), 1.0, 6.0, ((0, 8), (1, 4)))
    value_rows = gaussian(arg_keys[2], (ATTENTION_TOKENS, KV_HEADS * DH), 1.0, 6.0, ((0, 8), (1, 4)))
    break_bias = draw_break_bias(jax.random.fold_in(arg_keys[16], 71), 0)
    mixer_weight = gaussian(arg_keys[4], (HEADS * DH, D), (HEADS * DH) ** -0.5, 0.1875, ((0, 4),))
    mixer_gain = jnp.clip(1.0 + 0.18 * jax.random.normal(arg_keys[5], (D,), jnp.float32), 0.099609375, 1.8984375).astype(jnp.bfloat16)
    expert_input = gaussian(arg_keys[6], (TOKENS_B, D), 1.0, 6.0, ((0, 32),))
    expert_gain = jnp.clip(1.0 + 0.18 * jax.random.normal(arg_keys[7], (D,), jnp.float32), 0.099609375, 1.8984375).astype(jnp.bfloat16)
    route_ids_keys = jax.random.split(jax.random.fold_in(arg_keys[8], 1), TOKENS_B // TOK_B_DEV)
    route_ids_turns = jax.random.permutation(jax.random.fold_in(arg_keys[8], 3), TOKENS_B // TOK_B_DEV)
    route_ids = jax.vmap(lambda own, number: deal_out(jax.random.fold_in(arg_keys[8], 2), own, number, TOK_B_DEV, EXPERTS, TOPK, CAP, 1))(route_ids_keys, route_ids_turns).reshape((TOKENS_B, TOPK))
    route_weights = jnp.clip(jnp.exp(math.log(2.0) - 2.3025851 * jax.random.uniform(arg_keys[9], (TOKENS_B, TOPK), jnp.float32) ** block_scale(arg_keys[9], (TOKENS_B, TOPK), ((0, 32),), -0.2, 0.2)), 0.2, 2.0)
    expert_gate = gaussian(arg_keys[10], (EXPERTS, D, FF_E), D ** -0.5, 0.125, ((0, 8), (2, 4)))
    expert_up = gaussian(arg_keys[11], (EXPERTS, D, FF_E), D ** -0.5, 0.125, ((0, 8), (2, 4)))
    expert_down = gaussian(arg_keys[12], (EXPERTS, FF_E, D), FF_E ** -0.5, 0.125, ((0, 8), (1, 4)))
    shared_gate = gaussian(arg_keys[13], (D, SHARED_FF), D ** -0.5, 0.125)
    shared_up = gaussian(arg_keys[14], (D, SHARED_FF), D ** -0.5, 0.125)
    shared_down = gaussian(arg_keys[15], (SHARED_FF, D), SHARED_FF ** -0.5, 0.25)
    return dict(query_rows=query_rows, key_rows=key_rows, value_rows=value_rows, break_bias=break_bias, mixer_weight=mixer_weight, mixer_gain=mixer_gain, expert_input=expert_input, expert_gain=expert_gain, route_ids=route_ids, route_weights=route_weights, expert_gate=expert_gate, expert_up=expert_up, expert_down=expert_down, shared_gate=shared_gate, shared_up=shared_up, shared_down=shared_down)


norm_eps = 1e-06

def rms_scale(values, gain):
    values = values.astype(jnp.float32)
    scale = lax.rsqrt(lax.optimization_barrier(jnp.mean(values * values, axis=-1, keepdims=True)) + norm_eps)
    return (values * scale * gain.astype(jnp.float32)).astype(jnp.bfloat16)

def rounded(values):
    return lax.optimization_barrier(values.astype(jnp.bfloat16)).astype(jnp.float32)

def mixer_reference(query_rows, key_rows, value_rows, break_bias, mixer_weight, mixer_gain):
    groups = HEADS // KV_HEADS
    span_shards = N_EP // SEQS
    queries = query_rows.astype(jnp.float32).reshape(N_EP, TOK_A_DEV, KV_HEADS, groups, DH)
    keys = key_rows.astype(jnp.float32).reshape(N_EP, TOK_A_DEV, KV_HEADS, DH)
    values = value_rows.astype(jnp.float32).reshape(N_EP, TOK_A_DEV, KV_HEADS, DH)
    biases = break_bias.astype(jnp.float32).reshape(N_EP, TOK_A_DEV, HEADS)
    offsets = jnp.arange(TOK_A_DEV, dtype=jnp.int32)

    def query_block(device):
        query_block_rows = lax.dynamic_index_in_dim(queries, device, 0, keepdims=False)
        query_pos = device * TOK_A_DEV + offsets

        def visit(carry, shard):
            output, later = carry

            def compute(unused):
                key_block = lax.dynamic_index_in_dim(keys, shard, 0, keepdims=False)
                value_block = lax.dynamic_index_in_dim(values, shard, 0, keepdims=False)
                bias_block = lax.dynamic_index_in_dim(biases, shard, 0, keepdims=False)
                scores = jnp.einsum('rkgd,skd->kgrs', query_block_rows, key_block)
                scores = scores.reshape(HEADS, TOK_A_DEV, TOK_A_DEV) * DH ** (-0.5)
                scores = scores + bias_block.T[:, None, :]
                key_pos = shard * TOK_A_DEV + offsets
                visible = key_pos[None, :] < query_pos[:, None]
                keep = jnp.where(visible, -jax.nn.softplus(scores), 0.0)
                beyond = lax.cumsum(keep, axis=2, reverse=True) - keep
                weights = jnp.where(visible, jnp.exp(jax.nn.log_sigmoid(scores) + beyond), 0.0)
                weights = rounded(weights).reshape(KV_HEADS, groups, TOK_A_DEV, TOK_A_DEV)
                block_sum = jnp.einsum('kgrs,skd->kgrd', weights, value_block).reshape(HEADS, TOK_A_DEV, DH)
                return (output + jnp.exp(later)[:, :, None] * block_sum, later + lax.optimization_barrier(jnp.sum(keep, axis=2)))
            wanted = (shard <= device) & (shard // span_shards == device // span_shards)
            return (lax.cond(wanted, compute, lambda unused: (output, later), None), None)
        initial = (jnp.zeros((HEADS, TOK_A_DEV, DH), jnp.float32), jnp.zeros((HEADS, TOK_A_DEV), jnp.float32))
        (output, later), unused = lax.scan(visit, initial, jnp.arange(N_EP - 1, -1, -1, dtype=jnp.int32))
        return output.transpose(1, 0, 2).reshape(TOK_A_DEV, HEADS * DH)
    attended = lax.map(query_block, jnp.arange(N_EP, dtype=jnp.int32))
    attended = attended.reshape(ATTENTION_TOKENS, HEADS * DH).astype(jnp.bfloat16)
    group_width = HEADS * DH // N_TP
    projected = jnp.zeros((ATTENTION_TOKENS, D), jnp.float32)
    for group in range(N_TP):
        lower = group * group_width
        upper = lower + group_width
        projected = projected + rounded(jnp.dot(attended[:, lower:upper], mixer_weight[lower:upper], preferred_element_type=jnp.float32))
    return rms_scale(projected, mixer_gain)

def expert_reference(expert_input, expert_gain, route_ids, route_weights, expert_gate, expert_up, expert_down, shared_gate, shared_up, shared_down):
    normed = rms_scale(expert_input, expert_gain)
    padded = jnp.concatenate([normed, jnp.zeros((1, D), jnp.bfloat16)], axis=0)
    quarter = FF_E // N_TP
    slot_count = N_EP * N_TP * CAP

    def one_expert(routed, expert):
        named = route_ids == expert
        owners = jnp.nonzero(jnp.any(named, axis=1), size=slot_count, fill_value=TOKENS_B)[0].astype(jnp.int32)
        arrived = padded[owners]
        gate_proj = jnp.dot(arrived, expert_gate[expert], preferred_element_type=jnp.float32)
        up_proj = jnp.dot(arrived, expert_up[expert], preferred_element_type=jnp.float32)
        hidden = (jax.nn.silu(gate_proj) * up_proj).astype(jnp.bfloat16)
        down_matrix = expert_down[expert]
        output = jnp.zeros((slot_count, D), jnp.float32)
        for group in range(N_TP):
            lower = group * quarter
            upper = lower + quarter
            output = output + rounded(jnp.dot(hidden[:, lower:upper], down_matrix[lower:upper], preferred_element_type=jnp.float32))
        output = rounded(output)
        weight = lax.optimization_barrier(jnp.sum(jnp.where(named, route_weights, 0.0), axis=1))
        weight = jnp.concatenate([weight, jnp.zeros((1,), jnp.float32)], axis=0)
        return (routed.at[owners].add(weight[owners][:, None] * output), None)
    routed, unused = lax.scan(one_expert, jnp.zeros((TOKENS_B + 1, D), jnp.float32), jnp.arange(EXPERTS, dtype=jnp.int32))
    shared_hidden = (jax.nn.silu(jnp.dot(normed, shared_gate, preferred_element_type=jnp.float32)) * jnp.dot(normed, shared_up, preferred_element_type=jnp.float32)).astype(jnp.bfloat16)
    total = routed[:TOKENS_B] + jnp.dot(shared_hidden, shared_down, preferred_element_type=jnp.float32)
    return total.astype(jnp.bfloat16)

def reference(query_rows, key_rows, value_rows, break_bias, mixer_weight, mixer_gain, expert_input, expert_gain, route_ids, route_weights, expert_gate, expert_up, expert_down, shared_gate, shared_up, shared_down):
    mixer_out = mixer_reference(query_rows, key_rows, value_rows, break_bias, mixer_weight, mixer_gain)
    expert_out = expert_reference(expert_input, expert_gain, route_ids, route_weights, expert_gate, expert_up, expert_down, shared_gate, shared_up, shared_down)
    return (mixer_out, expert_out)
```

```python
import functools

import jax
import jax.numpy as jnp
from jax import lax
from jax.experimental import pallas as pl
from jax.experimental.pallas import tpu as pltpu
from jax.sharding import PartitionSpec as P

DH = 64
TOPK = 2
SEQS = 1
MESH = pl.DeviceIdType.MESH

norm_eps = 1e-06
F32 = jnp.float32
BF16 = jnp.bfloat16


def dot(left, right):
    return jnp.dot(left, right, preferred_element_type=F32)


def iota(shape, dim):
    return lax.broadcasted_iota(jnp.int32, shape, dim)


def joined(values):
    rows = values.shape[-2]
    flat = (-1, values.shape[-1])
    if rows % 16:
        return values.astype(F32).reshape(flat).astype(BF16)
    return values.reshape(flat)


def layer_kernel(
    cfg,
    query_ref,
    key_ref,
    value_ref,
    bias_ref,
    mixer_gain_ref,
    input_ref,
    expert_gain_ref,
    ids_ref,
    route_ref,
    mixer_hbm,
    gate_hbm,
    up_hbm,
    down_hbm,
    shared_gate_hbm,
    shared_up_hbm,
    shared_down_hbm,
    mixer_out_ref,
    expert_out_ref,
    arrived,
    outgoing,
    partial,
    from_core,
    from_x,
    returned,
    gate,
    up,
    down,
    shared_gate,
    shared_up,
    shared_down,
    mixer,
    kv,
    projected,
    mixer_core,
    mixer_x,
    output,
    later,
    queries,
    normed,
    mixing,
    shared_out,
    weight_sem,
    kv_recv,
    kv_chain,
    kv_pair,
    arrive_sem,
    send_sem,
    x_sem,
    core_sem,
    core2_sem,
    s1_sem,
    r1_sem,
    s2_sem,
    r2_sem,
    s3_sem,
    r3_sem,
    mixer_sem,
):
    ep_size, experts_local, capacity, heads, kv_heads = cfg
    group = lax.axis_index("ep").astype(jnp.int32)
    tp = lax.axis_index("tp").astype(jnp.int32)
    rows, kv_width = key_ref.shape
    tokens, width = input_ref.shape
    experts = experts_local * ep_size
    groups = heads // kv_heads
    span = ep_size // SEQS

    core_of, x_of = tp % 2, tp // 2
    core_peer = tp + 1 - 2 * core_of
    x_peer = x_of * -2 + core_of + 2
    mine = core_of * 2 + x_of
    slot_core = (1 - core_of) * 2 + x_of
    slot_x = core_of * 2 + 1 - x_of
    slot_diagonal = (1 - core_of) * 2 + 1 - x_of

    place = group % span
    base = group - place
    pair_of, chain_of = place % 2, place // 2
    pair = group + 1 - 2 * pair_of
    chains = span // 2
    above = jnp.where(chain_of + 1 < chains, group + 2, group)

    def remote(source, target, sent, received, ep, to):
        return pltpu.make_async_remote_copy(
            src_ref=source,
            dst_ref=target,
            send_sem=sent,
            recv_sem=received,
            device_id=(ep, to),
            device_id_type=MESH,
        )

    barrier = pltpu.get_barrier_semaphore()

    def greet(step, carry):
        other = (group + 1 + step) % ep_size
        pl.semaphore_signal(barrier, inc=1, device_id=(other, tp), device_id_type=MESH)
        return carry

    lax.fori_loop(0, ep_size - 1, greet, 0)
    for to in (core_peer, x_peer):
        pl.semaphore_signal(barrier, inc=1, device_id=(group, to), device_id_type=MESH)

    loads = []
    for source, target in (
        (mixer_hbm, mixer),
        (gate_hbm, gate),
        (up_hbm, up),
        (down_hbm, down),
        (shared_gate_hbm, shared_gate),
        (shared_up_hbm, shared_up),
        (shared_down_hbm, shared_down),
    ):
        load = pltpu.make_async_copy(source, target, weight_sem.at[len(loads)])
        load.start()
        loads.append(load)

    parts = -(-rows // (2 * kv_width))
    kv[group, 0:rows, 0:kv_width] = key_ref[...]
    kv[group, 0:rows, kv_width : 2 * kv_width] = value_ref[...]
    biases = jnp.concatenate([bias_ref[...].astype(F32), jnp.zeros((8 - heads, rows), F32)], axis=0)
    pieces = []
    for part in range(parts):
        piece = biases[:, part * 2 * kv_width : min(rows, (part + 1) * 2 * kv_width)]
        missing = 2 * kv_width - piece.shape[1]
        if missing:
            piece = jnp.concatenate([piece, jnp.zeros((8, missing), F32)], axis=1)
        pieces.append(piece)
    while len(pieces) % 2:
        pieces.append(jnp.zeros((8, 2 * kv_width), F32))
    kv[group, rows : rows + 8 * len(pieces), :] = jnp.concatenate(pieces, axis=0).astype(BF16)

    first_token = pl.multiple_of(tp * tokens, tokens)
    first_id = ids_ref[0:1, pl.ds(first_token, tokens)]
    second_id = ids_ref[1:2, pl.ds(first_token, tokens)]
    number = iota((experts, tokens), 0)
    is_first, is_second = number == first_id, number == second_id
    named = jnp.where(is_first | is_second, 1.0, 0.0).astype(BF16)
    weight = jnp.where(is_first, route_ref[0:1, :], jnp.where(is_second, route_ref[1:2, :], 0.0))
    earlier = (iota((tokens, tokens), 0) < iota((tokens, tokens), 1)).astype(F32).astype(BF16)
    before = dot(named, earlier).astype(BF16)
    slots = experts * capacity
    slot = iota((slots, experts), 0)
    owner = iota((slots, experts), 1) * capacity
    spread = ((slot >= owner) & (slot < owner + capacity)).astype(F32).astype(BF16)
    rank = (iota((slots, tokens), 0) % capacity).astype(F32)
    chosen = (dot(spread, named) > 0.5) & (dot(spread, before) == rank)
    mixing[...] = jnp.where(chosen, dot(spread, weight.astype(BF16)), 0.0).astype(BF16)
    chosen = jnp.where(chosen, 1.0, 0.0).astype(BF16)

    values = input_ref[...].astype(F32)
    scale = lax.rsqrt(jnp.mean(values * values, axis=-1, keepdims=True) + norm_eps)
    normed[...] = (values * scale * expert_gain_ref[...].astype(F32)).astype(BF16)
    tile = min(width, 512)
    for start in range(0, width, tile):
        block = dot(chosen, normed[:, start : start + tile])
        block = block.reshape(ep_size, experts_local, capacity, tile)
        outgoing[:, :, :, start : start + tile] = block.astype(BF16)
    arrived[mine, group] = outgoing[group]

    select = {}
    for head in range(heads):
        shape = (heads * DH, kv_width)
        inside = iota(shape, 1) - (head // groups) * DH
        picked = (iota(shape, 0) - head * DH == inside) & (inside >= 0) & (inside < DH)
        select[head] = picked.astype(F32)
        queries[head] = dot(query_ref[...], (select[head] * DH ** (-0.5)).astype(BF16)).astype(BF16)

    pl.semaphore_wait(barrier, ep_size + 1)

    def chain_copy(step):
        block = base + jnp.maximum(place - 2 * step, 0)
        return remote(kv.at[block], kv.at[block], kv_chain.at[step], kv_recv.at[block], above, tp)

    def pair_copy(step):
        block = base + jnp.maximum(place - 2 * step, 0)
        return remote(kv.at[block], kv.at[block], kv_pair.at[step], kv_recv.at[block], pair, tp)

    def await_kv(block):
        remote(kv.at[block], kv.at[block], kv_chain.at[0], kv_recv.at[block], pair, tp).wait_recv()

    @pl.when(chain_of + 1 < chains)
    def _():
        chain_copy(0).start()

    @pl.when(pair_of == 0)
    def _():
        pair_copy(0).start()

    def dispatch_copy(step):
        to = (group + ep_size - 1 - step) % ep_size
        return remote(
            outgoing.at[to], arrived.at[mine, group], send_sem.at[to], arrive_sem.at[mine, group], to, tp
        )

    def dispatch(step, carry):
        dispatch_copy(step).start()
        return carry

    def x_copy(source, block):
        return remote(source, arrived.at[mine, block], x_sem.at[block], arrive_sem.at[mine, block], group, x_peer)

    def core_copy(source, block):
        return remote(
            source, arrived.at[mine, block], core_sem.at[block], arrive_sem.at[mine, block], group, core_peer
        )

    def core2_copy(block):
        part = arrived.at[slot_x, block]
        return remote(part, part, core2_sem.at[block], arrive_sem.at[slot_x, block], group, core_peer)

    def await_rows(place_of, block):
        part = arrived.at[place_of, block]
        remote(part, part, core_sem.at[block], arrive_sem.at[place_of, block], group, x_peer).wait_recv()

    x_copy(outgoing.at[group], group).start()
    core_copy(outgoing.at[group], group).start()
    lax.fori_loop(0, group, dispatch, 0)

    @pl.when(chain_of == 0)
    def _():
        lax.fori_loop(group, ep_size - 1, dispatch, 0)

    row_of = iota((rows, rows), 0)
    column_of = iota((rows, rows), 1)
    after = (column_of < row_of).astype(F32).astype(BF16)

    def visit(block, head, diagonal):
        keys = kv[block, 0:rows, 0:kv_width]
        scores = lax.dot_general(
            queries[head], keys, (((1,), (1,)), ((), ())), preferred_element_type=F32
        )
        tail = kv[block, rows : rows + 8 * len(pieces), :].astype(F32)
        bias = []
        for part in range(parts):
            line = jnp.where(iota(tail.shape, 0) == head + 8 * part, tail, 0.0)
            line = jnp.sum(line, axis=0, keepdims=True)
            bias.append(line[:, : min(2 * kv_width, rows - part * 2 * kv_width)])
        scores = scores + jnp.concatenate(bias, axis=1)
        soft = jnp.log(1.0 + jnp.exp(-jnp.abs(scores)))
        keep = -(jnp.maximum(scores, 0.0) + soft)
        if diagonal:
            keep = jnp.where(column_of < row_of, keep, 0.0)
        high = keep.astype(BF16)
        low = (keep - high.astype(F32)).astype(BF16)
        beyond = dot(high, after) + dot(low, after)
        weights = jnp.exp(jnp.minimum(scores, 0.0) - soft + beyond)
        if diagonal:
            weights = jnp.where(column_of < row_of, weights, 0.0)
        total = beyond[:, 0:1] + keep[:, 0:1]
        summed = dot(weights.astype(BF16), kv[block, 0:rows, kv_width : 2 * kv_width])
        return summed, total

    def first_visit(head, carry):
        summed, total = visit(group, head, True)
        output[head] = summed
        later[head] = total
        return carry

    lax.fori_loop(0, heads, first_visit, 0)

    def attend(step, carry):
        @pl.when(step <= chain_of)
        def _():
            await_kv(base + jnp.maximum(place - 2 * step, 0))

            @pl.when(chain_of + 1 < chains)
            def _():
                chain_copy(step).start()

            pair_copy(step).start()

        @pl.when(step == chain_of)
        def _():
            lax.fori_loop(group, ep_size - 1, dispatch, 0)

        @pl.when(step <= place)
        def _():
            block = base + jnp.maximum(place - step, 0)

            @pl.when(step % 2 == 1)
            def _():
                await_kv(block)

            def next_visit(head, carry):
                summed, total = visit(block, head, False)
                passed = later[head]
                output[head] = output[head] + jnp.exp(passed) * summed
                later[head] = passed + total
                return carry

            lax.fori_loop(0, heads, next_visit, 0)

        block = (group + step) % ep_size
        await_rows(mine, block)
        x_copy(arrived.at[mine, block], block).start()
        core_copy(arrived.at[mine, block], block).start()
        return carry

    lax.fori_loop(1, ep_size, attend, 0)

    def forward(step):
        block = (group + 1 + step) % ep_size
        await_rows(slot_x, block)
        core2_copy(block).start()

    forward(0)

    attended = jnp.zeros((rows, heads * DH), F32)
    for head in range(heads):
        attended = attended + lax.dot_general(
            output[head].astype(BF16),
            select[head].astype(BF16),
            (((1,), (1,)), ((), ())),
            preferred_element_type=F32,
        )
    attended = attended.astype(BF16)
    for load in loads:
        load.wait()
    share = projected.shape[1]
    for to in range(projected.shape[0]):
        for start in range(0, width, tile):
            block = dot(attended[to * share : (to + 1) * share], mixer[:, start : start + tile])
            projected[(to % 2) * 2 + to // 2, :, start : start + tile] = block.astype(BF16)

    mixer_core_copy = remote(
        projected.at[pl.ds((1 - core_of) * 2, 2)], mixer_core, mixer_sem.at[0], mixer_sem.at[1], group, core_peer
    )
    mixer_x_copy = remote(
        projected.at[slot_x], mixer_x, mixer_sem.at[2], mixer_sem.at[3], group, x_peer
    )
    mixer_core_copy.start()

    def core_sum_copy(step):
        return remote(
            partial.at[step, pl.ds((1 - core_of) * 2, 2)],
            from_core.at[step],
            s1_sem.at[step],
            r1_sem.at[step],
            group,
            core_peer,
        )

    def x_sum_copy(step):
        return remote(
            partial.at[step, slot_x], from_x.at[step], s2_sem.at[step], r2_sem.at[step], group, x_peer
        )

    def return_copy(step):
        to = (group + 1 + step) % ep_size
        return remote(
            partial.at[step, mine], returned.at[group], s3_sem.at[to], r3_sem.at[group], to, tp
        )

    def work(step, carry):
        @pl.when(step < ep_size)
        def _():
            @pl.when(step + 1 < ep_size)
            def _():
                forward(step + 1)

            block = (group + 1 + step) % ep_size
            await_rows(slot_core, block)
            await_rows(slot_diagonal, block)
            for expert in range(experts_local):
                piece = joined(arrived[:, block, expert])
                gate_proj = dot(piece, gate[expert])
                up_proj = dot(piece, up[expert])
                hidden = (jax.nn.silu(gate_proj) * up_proj).astype(BF16)
                for start in range(0, width, tile):
                    part = dot(hidden, down[expert, :, start : start + tile])
                    part = part.reshape(4, capacity, tile).astype(BF16)
                    partial[step, :, expert, :, start : start + tile] = part
            core_sum_copy(step).start()

        @pl.when((step >= 1) & (step <= ep_size))
        def _():
            past = step - 1
            core_sum_copy(past).wait_recv()
            for slot_of, x_at in ((slot_x, 1 - x_of), (mine, x_of)):
                for expert in range(experts_local):
                    total = partial[past, slot_of, expert].astype(F32) + from_core[
                        past, x_at, expert
                    ].astype(F32)
                    partial[past, slot_of, expert] = total.astype(BF16)
            x_sum_copy(past).start()

        @pl.when(step == ep_size - 1)
        def _():
            mixer_core_copy.wait_recv()
            for slot_of, x_at in ((slot_x, 1 - x_of), (mine, x_of)):
                total = projected[slot_of].astype(F32) + mixer_core[x_at].astype(F32)
                projected[slot_of] = total.astype(BF16)
            mixer_x_copy.start()
            gate_proj = dot(normed[...], shared_gate[...])
            up_proj = dot(normed[...], shared_up[...])
            hidden = (jax.nn.silu(gate_proj) * up_proj).astype(BF16)
            for start in range(0, width, tile):
                shared_out[:, start : start + tile] = dot(hidden, shared_down[:, start : start + tile])

        @pl.when(step >= 2)
        def _():
            past = step - 2
            x_sum_copy(past).wait_recv()
            for expert in range(experts_local):
                total = partial[past, mine, expert].astype(F32) + from_x[past, expert].astype(F32)
                partial[past, mine, expert] = total.astype(BF16)

            @pl.when(past < ep_size - 1)
            def _():
                return_copy(past).start()

        return carry

    lax.fori_loop(0, ep_size + 2, work, 0)
    returned[group] = partial[ep_size - 1, mine]

    mixer_x_copy.wait_recv()
    total = projected[mine].astype(F32) + mixer_x[...].astype(F32)
    scale = lax.rsqrt(jnp.mean(total * total, axis=-1, keepdims=True) + norm_eps)
    mixer_out_ref[...] = (total * scale * mixer_gain_ref[...].astype(F32)).astype(BF16)

    def await_return(step, carry):
        block = (group + 1 + step) % ep_size
        remote(
            returned.at[block], returned.at[block], s3_sem.at[block], r3_sem.at[block], block, tp
        ).wait_recv()
        return carry

    lax.fori_loop(0, ep_size - 1, await_return, 0)
    for start in range(0, width, tile):
        results = joined(returned[:, :, :, start : start + tile])
        mixed = lax.dot_general(
            mixing[...], results, (((0,), (0,)), ((), ())), preferred_element_type=F32
        )
        expert_out_ref[:, start : start + tile] = (
            mixed + shared_out[:, start : start + tile]
        ).astype(BF16)

    @pl.when(chain_of + 1 < chains)
    def _():
        def done(step, carry):
            chain_copy(step).wait_send()
            return carry

        lax.fori_loop(0, chain_of + 1, done, 0)

    @pl.when(pair_of == 0)
    def _():
        pair_copy(0).wait_send()

    def pair_done(step, carry):
        pair_copy(step).wait_send()
        return carry

    lax.fori_loop(1, chain_of + 1, pair_done, 0)

    def sent(step, carry):
        dispatch_copy(step).wait_send()
        return_copy(step).wait_send()
        return carry

    lax.fori_loop(0, ep_size - 1, sent, 0)

    def forwarded(block, carry):
        x_copy(arrived.at[mine, block], block).wait_send()
        core_copy(arrived.at[mine, block], block).wait_send()
        core2_copy(block).wait_send()
        core_sum_copy(block).wait_send()
        x_sum_copy(block).wait_send()
        return carry

    lax.fori_loop(0, ep_size, forwarded, 0)
    mixer_core_copy.wait_send()
    mixer_x_copy.wait_send()


def on_device(
    query_rows,
    key_rows,
    value_rows,
    break_bias,
    mixer_weight,
    mixer_gain,
    expert_input,
    expert_gain,
    route_ids,
    route_weights,
    expert_gate,
    expert_up,
    expert_down,
    shared_gate,
    shared_up,
    shared_down,
):
    rows = query_rows.shape[0]
    heads = query_rows.shape[1] // DH
    kv_width = key_rows.shape[1]
    kv_heads = kv_width // DH
    ep_size = lax.axis_size("ep")
    tp_size = lax.axis_size("tp")
    tokens, width = expert_input.shape
    experts_local, _, hidden = expert_gate.shape
    capacity = 2 * tokens * TOPK // (experts_local * ep_size)
    slots = experts_local * ep_size * capacity
    parts = -(-rows // (2 * kv_width))
    block_rows = rows + 8 * (parts + parts % 2)
    share = rows // tp_size
    cfg = (ep_size, experts_local, capacity, heads, kv_heads)
    piece = (experts_local, capacity, width)
    vmem = pl.BlockSpec(memory_space=pltpu.VMEM)
    hbm = pl.BlockSpec(memory_space=pl.ANY)
    dma = pltpu.SemaphoreType.DMA
    return pl.pallas_call(
        functools.partial(layer_kernel, cfg),
        out_shape=(
            jax.ShapeDtypeStruct((share, width), BF16),
            jax.ShapeDtypeStruct((tokens, width), BF16),
        ),
        in_specs=[vmem] * 9 + [hbm] * 7,
        out_specs=(vmem, vmem),
        scratch_shapes=[
            pltpu.VMEM((tp_size, ep_size) + piece, BF16),
            pltpu.VMEM((ep_size,) + piece, BF16),
            pltpu.VMEM((ep_size, tp_size) + piece, BF16),
            pltpu.VMEM((ep_size, 2) + piece, BF16),
            pltpu.VMEM((ep_size,) + piece, BF16),
            pltpu.VMEM((ep_size,) + piece, BF16),
            pltpu.VMEM(expert_gate.shape, BF16),
            pltpu.VMEM(expert_up.shape, BF16),
            pltpu.VMEM(expert_down.shape, BF16),
            pltpu.VMEM(shared_gate.shape, BF16),
            pltpu.VMEM(shared_up.shape, BF16),
            pltpu.VMEM(shared_down.shape, BF16),
            pltpu.VMEM(mixer_weight.shape, BF16),
            pltpu.VMEM((ep_size, block_rows, 2 * kv_width), BF16),
            pltpu.VMEM((tp_size, share, width), BF16),
            pltpu.VMEM((2, share, width), BF16),
            pltpu.VMEM((share, width), BF16),
            pltpu.VMEM((heads, rows, kv_width), F32),
            pltpu.VMEM((heads, rows, 1), F32),
            pltpu.VMEM((heads, rows, kv_width), BF16),
            pltpu.VMEM((tokens, width), BF16),
            pltpu.VMEM((slots, tokens), BF16),
            pltpu.VMEM((tokens, width), F32),
            dma((7,)),
            dma((ep_size,)),
            dma((ep_size,)),
            dma((ep_size,)),
            dma((tp_size, ep_size)),
            dma((ep_size,)),
            dma((ep_size,)),
            dma((ep_size,)),
            dma((ep_size,)),
            dma((ep_size,)),
            dma((ep_size,)),
            dma((ep_size,)),
            dma((ep_size,)),
            dma((ep_size,)),
            dma((ep_size,)),
            dma((4,)),
        ],
        compiler_params=pltpu.CompilerParams(
            collective_id=0, has_side_effects=True, vmem_limit_bytes=67043328
        ),
        name="layer",
    )(
        query_rows,
        key_rows,
        value_rows,
        break_bias.T,
        mixer_gain.reshape(1, -1),
        expert_input,
        expert_gain.reshape(1, -1),
        route_ids.T,
        route_weights.T,
        mixer_weight,
        expert_gate,
        expert_up,
        expert_down,
        shared_gate,
        shared_up,
        shared_down,
    )


def solution(mesh):
    return jax.shard_map(
        on_device,
        mesh=mesh,
        in_specs=(
            P("ep", "tp"),
            P("ep", "tp"),
            P("ep", "tp"),
            P("ep", "tp"),
            P("tp", None),
            P(),
            P(("ep", "tp"), None),
            P(),
            P("ep", None),
            P(("ep", "tp"), None),
            P("ep", None, "tp"),
            P("ep", None, "tp"),
            P("ep", "tp", None),
            P(),
            P(),
            P(),
        ),
        out_specs=(P(("ep", "tp"), None), P(("ep", "tp"), None)),
        check_vma=False,
    )
```

```python
import functools

import jax
import jax.numpy as jnp
from jax import lax
from jax.experimental import pallas as pl
from jax.experimental.pallas import tpu as pltpu
from jax.sharding import PartitionSpec as P

DH = 64
TOPK = 2
SEQS = 1
MESH = pl.DeviceIdType.MESH

norm_eps = 1e-06
F32 = jnp.float32
BF16 = jnp.bfloat16


def dot(left, right):
    return jnp.dot(left, right, preferred_element_type=F32)


def iota(shape, dim):
    return lax.broadcasted_iota(jnp.int32, shape, dim)


def as_row(ref):
    values = ref[...].astype(F32)
    return jnp.concatenate([values[at : at + 1] for at in range(values.shape[0])], axis=1)


def joined(values):
    rows = values.shape[-2]
    flat = (-1, values.shape[-1])
    if rows % 16:
        return values.astype(F32).reshape(flat).astype(BF16)
    return values.reshape(flat)


def layer_kernel(
    cfg,
    query_ref,
    key_ref,
    value_ref,
    bias_ref,
    mixer_gain_ref,
    input_ref,
    expert_gain_ref,
    ids_ref,
    route_ref,
    mixer_hbm,
    gate_hbm,
    up_hbm,
    down_hbm,
    shared_gate_hbm,
    shared_up_hbm,
    shared_down_hbm,
    mixer_out_ref,
    expert_out_ref,
    arrived,
    raw,
    info,
    crossing,
    partial,
    from_core,
    from_x,
    returned,
    gate,
    up,
    down,
    shared_gate,
    shared_up,
    shared_down,
    mixer,
    kv,
    projected,
    mixer_core,
    mixer_x,
    output,
    later,
    queries,
    normed,
    mixing,
    shared_out,
    weight_sem,
    kv_recv,
    kv_chain,
    kv_pair,
    arrive_sem,
    raw_recv,
    raw_up,
    raw_down,
    info_recv,
    info_up,
    info_down,
    y_sem,
    x_sem,
    core_sem,
    core2_sem,
    s1_sem,
    r1_sem,
    s2_sem,
    r2_sem,
    s3_sem,
    r3_sem,
    mixer_sem,
):
    ep_size, experts_local, capacity, heads, kv_heads = cfg
    group = lax.axis_index("ep").astype(jnp.int32)
    tp = lax.axis_index("tp").astype(jnp.int32)
    rows, kv_width = key_ref.shape
    tokens, width = input_ref.shape
    experts = experts_local * ep_size
    groups = heads // kv_heads
    span = ep_size // SEQS

    core_of, x_of = tp % 2, tp // 2
    core_peer = tp + 1 - 2 * core_of
    x_peer = x_of * -2 + core_of + 2
    mine = core_of * 2 + x_of
    slot_core = (1 - core_of) * 2 + x_of
    slot_x = core_of * 2 + 1 - x_of
    slot_diagonal = (1 - core_of) * 2 + 1 - x_of

    place = group % span
    base = group - place
    pair_of, chain_of = place % 2, place // 2
    pair = group + 1 - 2 * pair_of
    chains = span // 2
    above = jnp.where(chain_of + 1 < chains, group + 2, group)
    line, lines = group // 2, ep_size // 2
    upper = jnp.where(line + 1 < lines, group + 2, group)
    lower = jnp.where(line > 0, group - 2, group)

    def remote(source, target, sent, received, ep, to):
        return pltpu.make_async_remote_copy(
            src_ref=source,
            dst_ref=target,
            send_sem=sent,
            recv_sem=received,
            device_id=(ep, to),
            device_id_type=MESH,
        )

    barrier = pltpu.get_barrier_semaphore()

    def greet(step, carry):
        other = (group + 1 + step) % ep_size
        pl.semaphore_signal(barrier, inc=1, device_id=(other, tp), device_id_type=MESH)
        return carry

    lax.fori_loop(0, ep_size - 1, greet, 0)
    for to in (core_peer, x_peer):
        pl.semaphore_signal(barrier, inc=1, device_id=(group, to), device_id_type=MESH)

    loads = []
    for source, target in (
        (mixer_hbm, mixer),
        (gate_hbm, gate),
        (up_hbm, up),
        (down_hbm, down),
        (shared_gate_hbm, shared_gate),
        (shared_up_hbm, shared_up),
        (shared_down_hbm, shared_down),
    ):
        load = pltpu.make_async_copy(source, target, weight_sem.at[len(loads)])
        load.start()
        loads.append(load)

    parts = -(-rows // (2 * kv_width))
    kv[group, 0:rows, 0:kv_width] = key_ref[...]
    kv[group, 0:rows, kv_width : 2 * kv_width] = value_ref[...]
    biases = jnp.concatenate([bias_ref[...].astype(F32), jnp.zeros((8 - heads, rows), F32)], axis=0)
    pieces = []
    for part in range(parts):
        piece = biases[:, part * 2 * kv_width : min(rows, (part + 1) * 2 * kv_width)]
        missing = 2 * kv_width - piece.shape[1]
        if missing:
            piece = jnp.concatenate([piece, jnp.zeros((8, missing), F32)], axis=1)
        pieces.append(piece)
    while len(pieces) % 2:
        pieces.append(jnp.zeros((8, 2 * kv_width), F32))
    kv[group, rows : rows + 8 * len(pieces), :] = jnp.concatenate(pieces, axis=0).astype(BF16)

    first_token = pl.multiple_of(tp * tokens, tokens)
    first_id = ids_ref[0:1, pl.ds(first_token, tokens)]
    second_id = ids_ref[1:2, pl.ds(first_token, tokens)]
    number = iota((experts, tokens), 0)
    is_first, is_second = number == first_id, number == second_id
    named = jnp.where(is_first | is_second, 1.0, 0.0).astype(BF16)
    weight = jnp.where(is_first, route_ref[0:1, :], jnp.where(is_second, route_ref[1:2, :], 0.0))
    earlier = (iota((tokens, tokens), 0) < iota((tokens, tokens), 1)).astype(F32).astype(BF16)
    before = dot(named, earlier)
    info[line] = jnp.concatenate(
        [
            first_id.astype(F32),
            jnp.sum(jnp.where(is_first, before, 0.0), axis=0, keepdims=True),
            second_id.astype(F32),
            jnp.sum(jnp.where(is_second, before, 0.0), axis=0, keepdims=True),
            jnp.zeros((4, tokens), F32),
        ],
        axis=0,
    )
    values = input_ref[...].astype(F32)
    scale = lax.rsqrt(jnp.mean(values * values, axis=-1, keepdims=True) + norm_eps)
    values = (values * scale * as_row(expert_gain_ref)).astype(BF16)
    normed[...] = values
    raw[line] = values
    tile = min(width, 512)

    half = experts_local * capacity
    row = iota((2 * half, tokens), 0)
    own_half = row < half
    row_expert = jnp.where(own_half, row // capacity + group * experts_local, row // capacity + (pair - 1) * experts_local)
    row_expert = row_expert.astype(F32)
    row_rank = (row % capacity).astype(F32)

    def pick(at):
        told = info[at]
        wanted = ((row_expert == told[0:1]) & (row_rank == told[1:2])) | (
            (row_expert == told[2:3]) & (row_rank == told[3:4])
        )
        wanted = jnp.where(wanted, 1.0, 0.0).astype(BF16)
        for start in range(0, width, tile):
            block = dot(wanted, raw[at, :, start : start + tile])
            block = block.reshape(2, experts_local, capacity, tile).astype(BF16)
            arrived[mine, 2 * at + pair_of, :, :, start : start + tile] = block[0]
            crossing[at, :, :, start : start + tile] = block[1]

    pick(line)

    select = {}
    for head in range(heads):
        shape = (heads * DH, kv_width)
        inside = iota(shape, 1) - (head // groups) * DH
        picked = (iota(shape, 0) - head * DH == inside) & (inside >= 0) & (inside < DH)
        select[head] = picked.astype(F32)
        queries[head] = dot(query_ref[...], (select[head] * DH ** (-0.5)).astype(BF16)).astype(BF16)

    slots = experts * capacity
    slot = iota((slots, experts), 0)
    owner = iota((slots, experts), 1) * capacity
    spread = ((slot >= owner) & (slot < owner + capacity)).astype(F32).astype(BF16)
    rank = (iota((slots, tokens), 0) % capacity).astype(F32)
    chosen = (dot(spread, named) > 0.5) & (dot(spread, before.astype(BF16)) == rank)
    mixing[...] = jnp.where(chosen, dot(spread, weight.astype(BF16)), 0.0).astype(BF16)

    pl.semaphore_wait(barrier, ep_size + 1)

    def chain_copy(step):
        block = base + jnp.maximum(place - 2 * step, 0)
        return remote(kv.at[block], kv.at[block], kv_chain.at[step], kv_recv.at[block], above, tp)

    def pair_copy(step):
        block = base + jnp.maximum(place - 2 * step, 0)
        return remote(kv.at[block], kv.at[block], kv_pair.at[step], kv_recv.at[block], pair, tp)

    def await_kv(block):
        remote(kv.at[block], kv.at[block], kv_chain.at[0], kv_recv.at[block], pair, tp).wait_recv()

    @pl.when(chain_of + 1 < chains)
    def _():
        chain_copy(0).start()

    @pl.when(pair_of == 0)
    def _():
        pair_copy(0).start()

    def raw_copies(at, to, raw_sent, info_sent):
        return (
            remote(raw.at[at], raw.at[at], raw_sent.at[at], raw_recv.at[at], to, tp),
            remote(info.at[at], info.at[at], info_sent.at[at], info_recv.at[at], to, tp),
        )

    def send_up(at):
        @pl.when(line + 1 < lines)
        def _():
            for copy in raw_copies(at, upper, raw_up, info_up):
                copy.start()

    def send_down(at):
        @pl.when(line > 0)
        def _():
            for copy in raw_copies(at, lower, raw_down, info_down):
                copy.start()

    def y_copy(at):
        block = 2 * at + pair_of
        return remote(crossing.at[at], arrived.at[mine, block], y_sem.at[at], arrive_sem.at[mine, block], pair, tp)

    def x_copy(source, block):
        return remote(source, arrived.at[mine, block], x_sem.at[block], arrive_sem.at[mine, block], group, x_peer)

    def core_copy(source, block):
        return remote(
            source, arrived.at[mine, block], core_sem.at[block], arrive_sem.at[mine, block], group, core_peer
        )

    def core2_copy(block):
        part = arrived.at[slot_x, block]
        return remote(part, part, core2_sem.at[block], arrive_sem.at[slot_x, block], group, core_peer)

    def await_rows(place_of, block):
        part = arrived.at[place_of, block]
        remote(part, part, core_sem.at[block], arrive_sem.at[place_of, block], group, x_peer).wait_recv()

    def pass_on(block):
        x_copy(arrived.at[mine, block], block).start()
        core_copy(arrived.at[mine, block], block).start()

    def cross(at):
        block = 2 * at + 1 - pair_of
        await_rows(mine, block)
        pass_on(block)

    def take(at):
        pick(at)
        pass_on(2 * at + pair_of)
        y_copy(at).start()

    pass_on(group)
    y_copy(line).start()
    send_down(line)

    @pl.when(chain_of == 0)
    def _():
        send_up(line)

    row_of = iota((rows, rows), 0)
    column_of = iota((rows, rows), 1)
    after = (column_of < row_of).astype(F32).astype(BF16)

    def visit(block, head, diagonal):
        keys = kv[block, 0:rows, 0:kv_width]
        scores = lax.dot_general(
            queries[head], keys, (((1,), (1,)), ((), ())), preferred_element_type=F32
        )
        tail = kv[block, rows : rows + 8 * len(pieces), :].astype(F32)
        bias = []
        for part in range(parts):
            line = jnp.where(iota(tail.shape, 0) == head + 8 * part, tail, 0.0)
            line = jnp.sum(line, axis=0, keepdims=True)
            bias.append(line[:, : min(2 * kv_width, rows - part * 2 * kv_width)])
        scores = scores + jnp.concatenate(bias, axis=1)
        soft = jnp.log(1.0 + jnp.exp(-jnp.abs(scores)))
        keep = -(jnp.maximum(scores, 0.0) + soft)
        if diagonal:
            keep = jnp.where(column_of < row_of, keep, 0.0)
        high = keep.astype(BF16)
        low = (keep - high.astype(F32)).astype(BF16)
        beyond = dot(high, after) + dot(low, after)
        weights = jnp.exp(jnp.minimum(scores, 0.0) - soft + beyond)
        if diagonal:
            weights = jnp.where(column_of < row_of, weights, 0.0)
        total = beyond[:, 0:1] + keep[:, 0:1]
        summed = dot(weights.astype(BF16), kv[block, 0:rows, kv_width : 2 * kv_width])
        return summed, total

    def first_visit(head, carry):
        summed, total = visit(group, head, True)
        output[head] = summed
        later[head] = total
        return carry

    lax.fori_loop(0, heads, first_visit, 0)

    def exchange(step):
        @pl.when(step == 1)
        def _():
            cross(line)

        @pl.when(step > 2)
        def _():
            at = jnp.where(step % 2 == 1, line + step // 2, line - (step - 2) // 2)

            @pl.when((at >= 0) & (at < lines))
            def _():
                cross(jnp.clip(at, 0, lines - 1))

        @pl.when(step > 1)
        def _():
            at = jnp.where(step % 2 == 0, line + step // 2, line - step // 2)
            at_in = jnp.clip(at, 0, lines - 1)

            @pl.when((at >= 0) & (at < lines))
            def _():
                for copy in raw_copies(at_in, upper, raw_up, info_up):
                    copy.wait_recv()

            @pl.when((at > line) & (at < lines))
            def _():
                send_down(at_in)

            @pl.when((at >= 0) & (at < line))
            def _():
                send_up(at_in)

            @pl.when((at >= 0) & (at < lines))
            def _():
                take(at_in)

    def attend(step, carry):
        @pl.when(step <= chain_of)
        def _():
            await_kv(base + jnp.maximum(place - 2 * step, 0))

            @pl.when(chain_of + 1 < chains)
            def _():
                chain_copy(step).start()

            pair_copy(step).start()

        @pl.when(step == chain_of)
        def _():
            send_up(line)

        @pl.when(line < lines - 1)
        def _():
            exchange(step)

        @pl.when(step <= place)
        def _():
            block = base + jnp.maximum(place - step, 0)

            @pl.when(step % 2 == 1)
            def _():
                await_kv(block)

            def next_visit(head, carry):
                summed, total = visit(block, head, False)
                passed = later[head]
                output[head] = output[head] + jnp.exp(passed) * summed
                later[head] = passed + total
                return carry

            lax.fori_loop(0, heads, next_visit, 0)

        @pl.when(line == lines - 1)
        def _():
            exchange(step)

        return carry

    lax.fori_loop(1, ep_size, attend, 0)
    last = line - (ep_size - 1) // 2

    def block_of(step):
        index = step // 2
        both = jnp.minimum(line, lines - 1 - line)
        near = jnp.where(index % 2 == 0, line - index // 2 - 1, line + index // 2 + 1)
        far = index - both + 1
        far = jnp.where(line > lines - 1 - line, line - far, line + far)
        at = jnp.where(index < 2 * both, near, far)
        at = jnp.where(index < lines - 1, at, line)
        side = jnp.where(index < lines - 1, (pair_of + step) % 2, (pair_of + step + 1) % 2)
        return jnp.clip(at, 0, lines - 1) * 2 + side

    def forward(step):
        block = block_of(step)
        await_rows(slot_x, block)
        core2_copy(block).start()

    forward(0)

    attended = jnp.zeros((rows, heads * DH), F32)
    for head in range(heads):
        attended = attended + lax.dot_general(
            output[head].astype(BF16),
            select[head].astype(BF16),
            (((1,), (1,)), ((), ())),
            preferred_element_type=F32,
        )
    attended = attended.astype(BF16)
    for load in loads:
        load.wait()
    share = projected.shape[1]
    for to in range(projected.shape[0]):
        for start in range(0, width, tile):
            block = dot(attended[to * share : (to + 1) * share], mixer[:, start : start + tile])
            projected[(to % 2) * 2 + to // 2, :, start : start + tile] = block.astype(BF16)

    mixer_core_copy = remote(
        projected.at[pl.ds((1 - core_of) * 2, 2)], mixer_core, mixer_sem.at[0], mixer_sem.at[1], group, core_peer
    )
    mixer_x_copy = remote(
        projected.at[slot_x], mixer_x, mixer_sem.at[2], mixer_sem.at[3], group, x_peer
    )
    mixer_core_copy.start()

    ring = partial.shape[0]

    def core_sum_copy(step):
        return remote(
            partial.at[step % ring, pl.ds((1 - core_of) * 2, 2)],
            from_core.at[step],
            s1_sem.at[step],
            r1_sem.at[step],
            group,
            core_peer,
        )

    def x_sum_copy(step):
        return remote(
            partial.at[step % ring, slot_x], from_x.at[step], s2_sem.at[step], r2_sem.at[step], group, x_peer
        )

    def return_copy(step):
        to = block_of(step)
        return remote(
            partial.at[step % ring, mine], returned.at[group], s3_sem.at[to], r3_sem.at[group], to, tp
        )

    def left(step):
        core_sum_copy(step).wait_send()
        x_sum_copy(step).wait_send()

        @pl.when(step < ep_size - 1)
        def _():
            return_copy(step).wait_send()

    def work(step, carry):
        @pl.when(step < ep_size)
        def _():
            @pl.when((step == 1) & (last >= 0))
            def _():
                cross(jnp.maximum(last, 0))

            @pl.when(step + 1 < ep_size)
            def _():
                forward(step + 1)

            block = block_of(step)
            await_rows(slot_core, block)
            await_rows(slot_diagonal, block)

            @pl.when(step >= ring)
            def _():
                left(jnp.maximum(step - ring, 0))

            for expert in range(experts_local):
                piece = joined(arrived[:, block, expert])
                gate_proj = dot(piece, gate[expert])
                up_proj = dot(piece, up[expert])
                hidden = (jax.nn.silu(gate_proj) * up_proj).astype(BF16)
                for start in range(0, width, tile):
                    part = dot(hidden, down[expert, :, start : start + tile])
                    part = part.reshape(4, capacity, tile).astype(BF16)
                    partial[step % ring, :, expert, :, start : start + tile] = part
            core_sum_copy(step).start()

        @pl.when((step >= 1) & (step <= ep_size))
        def _():
            past = step - 1
            core_sum_copy(past).wait_recv()
            for slot_of, x_at in ((slot_x, 1 - x_of), (mine, x_of)):
                for expert in range(experts_local):
                    total = partial[past % ring, slot_of, expert].astype(F32) + from_core[
                        past, x_at, expert
                    ].astype(F32)
                    partial[past % ring, slot_of, expert] = total.astype(BF16)
            x_sum_copy(past).start()

        @pl.when(step == ep_size - 1)
        def _():
            mixer_core_copy.wait_recv()
            for slot_of, x_at in ((slot_x, 1 - x_of), (mine, x_of)):
                total = projected[slot_of].astype(F32) + mixer_core[x_at].astype(F32)
                projected[slot_of] = total.astype(BF16)
            mixer_x_copy.start()
            gate_proj = dot(normed[...], shared_gate[...])
            up_proj = dot(normed[...], shared_up[...])
            hidden = (jax.nn.silu(gate_proj) * up_proj).astype(BF16)
            for start in range(0, width, tile):
                shared_out[:, start : start + tile] = dot(hidden, shared_down[:, start : start + tile])

        @pl.when(step >= 2)
        def _():
            past = step - 2
            x_sum_copy(past).wait_recv()
            for expert in range(experts_local):
                total = partial[past % ring, mine, expert].astype(F32) + from_x[past, expert].astype(F32)
                partial[past % ring, mine, expert] = total.astype(BF16)

            @pl.when(past < ep_size - 1)
            def _():
                return_copy(past).start()

        return carry

    lax.fori_loop(0, ep_size + 2, work, 0)
    returned[group] = partial[(ep_size - 1) % ring, mine]

    mixer_x_copy.wait_recv()
    total = projected[mine].astype(F32) + mixer_x[...].astype(F32)
    scale = lax.rsqrt(jnp.mean(total * total, axis=-1, keepdims=True) + norm_eps)
    mixer_out_ref[...] = (total * scale * as_row(mixer_gain_ref)).astype(BF16)

    def await_return(step, carry):
        block = (group + 1 + step) % ep_size
        remote(
            returned.at[block], returned.at[block], s3_sem.at[block], r3_sem.at[block], block, tp
        ).wait_recv()
        return carry

    lax.fori_loop(0, ep_size - 1, await_return, 0)
    for start in range(0, width, tile):
        results = joined(returned[:, :, :, start : start + tile])
        mixed = lax.dot_general(
            mixing[...], results, (((0,), (0,)), ((), ())), preferred_element_type=F32
        )
        expert_out_ref[:, start : start + tile] = (
            mixed + shared_out[:, start : start + tile]
        ).astype(BF16)

    @pl.when(chain_of + 1 < chains)
    def _():
        def done(step, carry):
            chain_copy(step).wait_send()
            return carry

        lax.fori_loop(0, chain_of + 1, done, 0)

    @pl.when(pair_of == 0)
    def _():
        pair_copy(0).wait_send()

    def pair_done(step, carry):
        pair_copy(step).wait_send()
        return carry

    lax.fori_loop(1, chain_of + 1, pair_done, 0)

    @pl.when(line + 1 < lines)
    def _():
        def done(at, carry):
            for copy in raw_copies(at, upper, raw_up, info_up):
                copy.wait_send()
            return carry

        lax.fori_loop(0, line + 1, done, 0)

    @pl.when(line > 0)
    def _():
        def done(at, carry):
            for copy in raw_copies(at, lower, raw_down, info_down):
                copy.wait_send()
            return carry

        lax.fori_loop(line, lines, done, 0)

    def crossed(at, carry):
        y_copy(at).wait_send()
        return carry

    lax.fori_loop(0, lines, crossed, 0)

    def forwarded(block, carry):
        x_copy(arrived.at[mine, block], block).wait_send()
        core_copy(arrived.at[mine, block], block).wait_send()
        core2_copy(block).wait_send()
        return carry

    lax.fori_loop(0, ep_size, forwarded, 0)

    def summed_up(step, carry):
        left(step)
        return carry

    lax.fori_loop(ep_size - ring, ep_size, summed_up, 0)
    mixer_core_copy.wait_send()
    mixer_x_copy.wait_send()


def hand_over_kernel(mixer_ref, expert_ref, mixer_out_ref, expert_out_ref):
    mixer_out_ref[...] = mixer_ref[...]
    expert_out_ref[...] = expert_ref[...]


def on_device(
    query_rows,
    key_rows,
    value_rows,
    break_bias,
    mixer_weight,
    mixer_gain,
    expert_input,
    expert_gain,
    route_ids,
    route_weights,
    expert_gate,
    expert_up,
    expert_down,
    shared_gate,
    shared_up,
    shared_down,
):
    rows = query_rows.shape[0]
    heads = query_rows.shape[1] // DH
    kv_width = key_rows.shape[1]
    kv_heads = kv_width // DH
    ep_size = lax.axis_size("ep")
    tp_size = lax.axis_size("tp")
    tokens, width = expert_input.shape
    experts_local, _, hidden = expert_gate.shape
    capacity = 2 * tokens * TOPK // (experts_local * ep_size)
    slots = experts_local * ep_size * capacity
    parts = -(-rows // (2 * kv_width))
    block_rows = rows + 8 * (parts + parts % 2)
    share = rows // tp_size
    lines = ep_size // 2
    cfg = (ep_size, experts_local, capacity, heads, kv_heads)
    piece = (experts_local, capacity, width)
    vmem = pl.BlockSpec(memory_space=pltpu.VMEM)
    hbm = pl.BlockSpec(memory_space=pl.ANY)
    dma = pltpu.SemaphoreType.DMA
    results = pl.pallas_call(
        functools.partial(layer_kernel, cfg),
        out_shape=(
            jax.ShapeDtypeStruct((share, width), BF16),
            jax.ShapeDtypeStruct((tokens, width), BF16),
        ),
        in_specs=[vmem] * 9 + [hbm] * 7,
        out_specs=(vmem, vmem),
        scratch_shapes=[
            pltpu.VMEM((tp_size, ep_size) + piece, BF16),
            pltpu.VMEM((lines, tokens, width), BF16),
            pltpu.VMEM((lines, 8, tokens), F32),
            pltpu.VMEM((lines,) + piece, BF16),
            pltpu.VMEM((min(ep_size, 8), tp_size) + piece, BF16),
            pltpu.VMEM((ep_size, 2) + piece, BF16),
            pltpu.VMEM((ep_size,) + piece, BF16),
            pltpu.VMEM((ep_size,) + piece, BF16),
            pltpu.VMEM(expert_gate.shape, BF16),
            pltpu.VMEM(expert_up.shape, BF16),
            pltpu.VMEM(expert_down.shape, BF16),
            pltpu.VMEM(shared_gate.shape, BF16),
            pltpu.VMEM(shared_up.shape, BF16),
            pltpu.VMEM(shared_down.shape, BF16),
            pltpu.VMEM(mixer_weight.shape, BF16),
            pltpu.VMEM((ep_size, block_rows, 2 * kv_width), BF16),
            pltpu.VMEM((tp_size, share, width), BF16),
            pltpu.VMEM((2, share, width), BF16),
            pltpu.VMEM((share, width), BF16),
            pltpu.VMEM((heads, rows, kv_width), F32),
            pltpu.VMEM((heads, rows, 1), F32),
            pltpu.VMEM((heads, rows, kv_width), BF16),
            pltpu.VMEM((tokens, width), BF16),
            pltpu.VMEM((slots, tokens), BF16),
            pltpu.VMEM((tokens, width), F32),
            dma((7,)),
            dma((ep_size,)),
            dma((ep_size,)),
            dma((ep_size,)),
            dma((tp_size, ep_size)),
            dma((lines,)),
            dma((lines,)),
            dma((lines,)),
            dma((lines,)),
            dma((lines,)),
            dma((lines,)),
            dma((lines,)),

            dma((ep_size,)),
            dma((ep_size,)),
            dma((ep_size,)),
            dma((ep_size,)),
            dma((ep_size,)),
            dma((ep_size,)),
            dma((ep_size,)),
            dma((ep_size,)),
            dma((ep_size,)),
            dma((4,)),
        ],
        compiler_params=pltpu.CompilerParams(
            collective_id=0, has_side_effects=True, vmem_limit_bytes=67043328
        ),
        name="layer",
    )(
        query_rows,
        key_rows,
        value_rows,
        break_bias.T,
        mixer_gain.reshape(-1, 128),
        expert_input,
        expert_gain.reshape(-1, 128),
        route_ids.T,
        route_weights.T,
        mixer_weight,
        expert_gate,
        expert_up,
        expert_down,
        shared_gate,
        shared_up,
        shared_down,
    )
    return pl.pallas_call(
        hand_over_kernel,
        out_shape=tuple(jax.ShapeDtypeStruct(result.shape, BF16) for result in results),
        in_specs=[vmem] * 2,
        out_specs=(vmem, vmem),
        name="hand_over",
    )(*results)


def solution(mesh):
    return jax.shard_map(
        on_device,
        mesh=mesh,
        in_specs=(
            P("ep", "tp"),
            P("ep", "tp"),
            P("ep", "tp"),
            P("ep", "tp"),
            P("tp", None),
            P(),
            P(("ep", "tp"), None),
            P(),
            P("ep", None),
            P(("ep", "tp"), None),
            P("ep", None, "tp"),
            P("ep", None, "tp"),
            P("ep", "tp", None),
            P(),
            P(),
            P(),
        ),
        out_specs=(P(("ep", "tp"), None), P(("ep", "tp"), None)),
        check_vma=False,
    )
```

```python
import functools

import jax
import jax.numpy as jnp
from jax import lax
from jax.experimental import pallas as pl
from jax.experimental.pallas import tpu as pltpu
from jax.sharding import PartitionSpec as P

DH = 64
TOPK = 2
SEQS = 1
MESH = pl.DeviceIdType.MESH

norm_eps = 1e-06
F32 = jnp.float32
BF16 = jnp.bfloat16


def dot(left, right):
    return jnp.dot(left, right, preferred_element_type=F32)


def iota(shape, dim):
    return lax.broadcasted_iota(jnp.int32, shape, dim)


def as_row(ref):
    values = ref[...].astype(F32)
    return jnp.concatenate([values[at : at + 1] for at in range(values.shape[0])], axis=1)


def joined(values):
    rows = values.shape[-2]
    flat = (-1, values.shape[-1])
    if rows % 16:
        return values.astype(F32).reshape(flat).astype(BF16)
    return values.reshape(flat)


def layer_kernel(
    cfg,
    query_ref,
    key_ref,
    value_ref,
    bias_ref,
    mixer_gain_ref,
    input_ref,
    expert_gain_ref,
    ids_ref,
    route_ref,
    mixer_hbm,
    gate_hbm,
    up_hbm,
    down_hbm,
    shared_gate_hbm,
    shared_up_hbm,
    shared_down_hbm,
    mixer_out_ref,
    expert_out_ref,
    arrived,
    raw,
    info,
    crossing,
    partial,
    from_core,
    from_x,
    returned,
    gate,
    up,
    down,
    shared_gate,
    shared_up,
    shared_down,
    mixer,
    kv,
    projected,
    mixer_core,
    mixer_x,
    output,
    later,
    queries,
    normed,
    mixing,
    shared_out,
    weight_sem,
    kv_recv,
    kv_chain,
    kv_pair,
    arrive_sem,
    raw_recv,
    raw_up,
    raw_down,
    info_recv,
    info_up,
    info_down,
    y_sem,
    x_sem,
    core_sem,
    core2_sem,
    s1_sem,
    r1_sem,
    s2_sem,
    r2_sem,
    s3_sem,
    r3_sem,
    mixer_sem,
):
    ep_size, experts_local, capacity, heads, kv_heads = cfg
    group = lax.axis_index("ep").astype(jnp.int32)
    tp = lax.axis_index("tp").astype(jnp.int32)
    rows, kv_width = key_ref.shape
    tokens, width = input_ref.shape
    experts = experts_local * ep_size
    groups = heads // kv_heads
    span = ep_size // SEQS

    core_of, x_of = tp % 2, tp // 2
    core_peer = tp + 1 - 2 * core_of
    x_peer = x_of * -2 + core_of + 2
    mine = core_of * 2 + x_of
    slot_core = (1 - core_of) * 2 + x_of
    slot_x = core_of * 2 + 1 - x_of
    slot_diagonal = (1 - core_of) * 2 + 1 - x_of

    place = group % span
    base = group - place
    pair_of, chain_of = place % 2, place // 2
    pair = group + 1 - 2 * pair_of
    chains = span // 2
    above = jnp.where(chain_of + 1 < chains, group + 2, group)
    line, lines = group // 2, ep_size // 2
    upper = jnp.where(line + 1 < lines, group + 2, group)
    lower = jnp.where(line > 0, group - 2, group)

    def remote(source, target, sent, received, ep, to):
        return pltpu.make_async_remote_copy(
            src_ref=source,
            dst_ref=target,
            send_sem=sent,
            recv_sem=received,
            device_id=(ep, to),
            device_id_type=MESH,
        )

    barrier = pltpu.get_barrier_semaphore()

    def greet(step, carry):
        other = (group + 1 + step) % ep_size
        pl.semaphore_signal(barrier, inc=1, device_id=(other, tp), device_id_type=MESH)
        return carry

    lax.fori_loop(0, ep_size - 1, greet, 0)
    for to in (core_peer, x_peer):
        pl.semaphore_signal(barrier, inc=1, device_id=(group, to), device_id_type=MESH)

    loads = []
    for source, target in (
        (mixer_hbm, mixer),
        (gate_hbm, gate),
        (up_hbm, up),
        (down_hbm, down),
        (shared_gate_hbm, shared_gate),
        (shared_up_hbm, shared_up),
        (shared_down_hbm, shared_down),
    ):
        load = pltpu.make_async_copy(source, target, weight_sem.at[len(loads)])
        load.start()
        loads.append(load)

    parts = -(-rows // (2 * kv_width))
    kv[group, 0:rows, 0:kv_width] = key_ref[...]
    kv[group, 0:rows, kv_width : 2 * kv_width] = value_ref[...]
    biases = jnp.concatenate([bias_ref[...].astype(F32), jnp.zeros((8 - heads, rows), F32)], axis=0)
    pieces = []
    for part in range(parts):
        piece = biases[:, part * 2 * kv_width : min(rows, (part + 1) * 2 * kv_width)]
        missing = 2 * kv_width - piece.shape[1]
        if missing:
            piece = jnp.concatenate([piece, jnp.zeros((8, missing), F32)], axis=1)
        pieces.append(piece)
    while len(pieces) % 2:
        pieces.append(jnp.zeros((8, 2 * kv_width), F32))
    kv[group, rows : rows + 8 * len(pieces), :] = jnp.concatenate(pieces, axis=0).astype(BF16)

    first_token = pl.multiple_of(tp * tokens, tokens)
    first_id = ids_ref[0:1, pl.ds(first_token, tokens)]
    second_id = ids_ref[1:2, pl.ds(first_token, tokens)]
    number = iota((experts, tokens), 0)
    is_first, is_second = number == first_id, number == second_id
    named = jnp.where(is_first | is_second, 1.0, 0.0).astype(BF16)
    weight = jnp.where(is_first, route_ref[0:1, :], jnp.where(is_second, route_ref[1:2, :], 0.0))
    earlier = (iota((tokens, tokens), 0) < iota((tokens, tokens), 1)).astype(F32).astype(BF16)
    before = dot(named, earlier)
    info[line] = jnp.concatenate(
        [
            first_id.astype(F32),
            jnp.sum(jnp.where(is_first, before, 0.0), axis=0, keepdims=True),
            second_id.astype(F32),
            jnp.sum(jnp.where(is_second, before, 0.0), axis=0, keepdims=True),
            jnp.zeros((4, tokens), F32),
        ],
        axis=0,
    )
    values = input_ref[...].astype(F32)
    scale = lax.rsqrt(jnp.mean(values * values, axis=-1, keepdims=True) + norm_eps)
    values = (values * scale * as_row(expert_gain_ref)).astype(BF16)
    normed[...] = values
    raw[line] = values
    tile = min(width, 512)

    half = experts_local * capacity
    row = iota((2 * half, tokens), 0)
    own_half = row < half
    row_expert = jnp.where(own_half, row // capacity + group * experts_local, row // capacity + (pair - 1) * experts_local)
    row_expert = row_expert.astype(F32)
    row_rank = (row % capacity).astype(F32)

    def pick(at):
        told = info[at]
        wanted = ((row_expert == told[0:1]) & (row_rank == told[1:2])) | (
            (row_expert == told[2:3]) & (row_rank == told[3:4])
        )
        wanted = jnp.where(wanted, 1.0, 0.0).astype(BF16)
        for start in range(0, width, tile):
            block = dot(wanted, raw[at, :, start : start + tile])
            block = block.reshape(2, experts_local, capacity, tile).astype(BF16)
            arrived[mine, 2 * at + pair_of, :, :, start : start + tile] = block[0]
            crossing[at, :, :, start : start + tile] = block[1]

    pick(line)

    select = {}
    for head in range(heads):
        shape = (heads * DH, kv_width)
        inside = iota(shape, 1) - (head // groups) * DH
        picked = (iota(shape, 0) - head * DH == inside) & (inside >= 0) & (inside < DH)
        select[head] = picked.astype(F32)
        queries[head] = dot(query_ref[...], (select[head] * DH ** (-0.5)).astype(BF16)).astype(BF16)

    slots = experts * capacity
    slot = iota((slots, experts), 0)
    owner = iota((slots, experts), 1) * capacity
    spread = ((slot >= owner) & (slot < owner + capacity)).astype(F32).astype(BF16)
    rank = (iota((slots, tokens), 0) % capacity).astype(F32)
    chosen = (dot(spread, named) > 0.5) & (dot(spread, before.astype(BF16)) == rank)
    mixing[...] = jnp.where(chosen, dot(spread, weight.astype(BF16)), 0.0).astype(BF16)

    pl.semaphore_wait(barrier, ep_size + 1)

    def chain_copy(step):
        block = base + jnp.maximum(place - 2 * step, 0)
        return remote(kv.at[block], kv.at[block], kv_chain.at[step], kv_recv.at[block], above, tp)

    def pair_copy(step):
        block = base + jnp.maximum(place - 2 * step, 0)
        return remote(kv.at[block], kv.at[block], kv_pair.at[step], kv_recv.at[block], pair, tp)

    def await_kv(block):
        remote(kv.at[block], kv.at[block], kv_chain.at[0], kv_recv.at[block], pair, tp).wait_recv()

    @pl.when(chain_of + 1 < chains)
    def _():
        chain_copy(0).start()

    @pl.when(pair_of == 0)
    def _():
        pair_copy(0).start()

    def raw_copies(at, to, raw_sent, info_sent):
        return (
            remote(raw.at[at], raw.at[at], raw_sent.at[at], raw_recv.at[at], to, tp),
            remote(info.at[at], info.at[at], info_sent.at[at], info_recv.at[at], to, tp),
        )

    def send_up(at):
        @pl.when(line + 1 < lines)
        def _():
            for copy in raw_copies(at, upper, raw_up, info_up):
                copy.start()

    def send_down(at):
        @pl.when(line > 0)
        def _():
            for copy in raw_copies(at, lower, raw_down, info_down):
                copy.start()

    def y_copy(at):
        block = 2 * at + pair_of
        return remote(crossing.at[at], arrived.at[mine, block], y_sem.at[at], arrive_sem.at[mine, block], pair, tp)

    def x_copy(source, block):
        return remote(source, arrived.at[mine, block], x_sem.at[block], arrive_sem.at[mine, block], group, x_peer)

    def core_copy(source, block):
        return remote(
            source, arrived.at[mine, block], core_sem.at[block], arrive_sem.at[mine, block], group, core_peer
        )

    def core2_copy(block):
        part = arrived.at[slot_x, block]
        return remote(part, part, core2_sem.at[block], arrive_sem.at[slot_x, block], group, core_peer)

    def await_rows(place_of, block):
        part = arrived.at[place_of, block]
        remote(part, part, core_sem.at[block], arrive_sem.at[place_of, block], group, x_peer).wait_recv()

    def pass_on(block):
        x_copy(arrived.at[mine, block], block).start()
        core_copy(arrived.at[mine, block], block).start()

    def cross(at):
        block = 2 * at + 1 - pair_of
        await_rows(mine, block)
        pass_on(block)

    def take(at):
        pick(at)
        pass_on(2 * at + pair_of)
        y_copy(at).start()

    pass_on(group)
    y_copy(line).start()
    send_down(line)

    @pl.when(chain_of == 0)
    def _():
        send_up(line)

    row_of = iota((rows, rows), 0)
    column_of = iota((rows, rows), 1)
    after = (column_of < row_of).astype(F32).astype(BF16)

    def visit(block, head, diagonal):
        keys = kv[block, 0:rows, 0:kv_width]
        scores = lax.dot_general(
            queries[head], keys, (((1,), (1,)), ((), ())), preferred_element_type=F32
        )
        tail = kv[block, rows : rows + 8 * len(pieces), :].astype(F32)
        bias = []
        for part in range(parts):
            line = jnp.where(iota(tail.shape, 0) == head + 8 * part, tail, 0.0)
            line = jnp.sum(line, axis=0, keepdims=True)
            bias.append(line[:, : min(2 * kv_width, rows - part * 2 * kv_width)])
        scores = scores + jnp.concatenate(bias, axis=1)
        soft = jnp.log(1.0 + jnp.exp(-jnp.abs(scores)))
        keep = -(jnp.maximum(scores, 0.0) + soft)
        if diagonal:
            keep = jnp.where(column_of < row_of, keep, 0.0)
        high = keep.astype(BF16)
        low = (keep - high.astype(F32)).astype(BF16)
        beyond = dot(high, after) + dot(low, after)
        weights = jnp.exp(jnp.minimum(scores, 0.0) - soft + beyond)
        if diagonal:
            weights = jnp.where(column_of < row_of, weights, 0.0)
        total = beyond[:, 0:1] + keep[:, 0:1]
        summed = dot(weights.astype(BF16), kv[block, 0:rows, kv_width : 2 * kv_width])
        return summed, total

    def first_visit(head, carry):
        summed, total = visit(group, head, True)
        output[head] = summed
        later[head] = total
        return carry

    lax.fori_loop(0, heads, first_visit, 0)

    def exchange(step):
        @pl.when(step == 1)
        def _():
            cross(line)

        @pl.when(step > 2)
        def _():
            at = jnp.where(step % 2 == 1, line + step // 2, line - (step - 2) // 2)

            @pl.when((at >= 0) & (at < lines))
            def _():
                cross(jnp.clip(at, 0, lines - 1))

        @pl.when(step > 1)
        def _():
            at = jnp.where(step % 2 == 0, line + step // 2, line - step // 2)
            at_in = jnp.clip(at, 0, lines - 1)

            @pl.when((at >= 0) & (at < lines))
            def _():
                for copy in raw_copies(at_in, upper, raw_up, info_up):
                    copy.wait_recv()

            @pl.when((at > line) & (at < lines))
            def _():
                send_down(at_in)

            @pl.when((at >= 0) & (at < line))
            def _():
                send_up(at_in)

            @pl.when((at >= 0) & (at < lines))
            def _():
                take(at_in)

    def block_of(step):
        index = step // 2
        middle = lines // 2
        lower_half = line < middle
        depth = jnp.where(lower_half, middle - line, line - middle + 1)
        turned = (index + depth) % middle
        across = jnp.where(lower_half, middle + turned, middle - 1 - turned)
        start = jnp.where(lower_half, 0, middle)
        beside = start + (line - start + 1 + index) % middle
        at = jnp.where(index < middle, across, beside)
        at = jnp.where(index < lines - 1, at, line)
        side = jnp.where(index < lines - 1, (pair_of + step) % 2, (pair_of + step + 1) % 2)
        return jnp.clip(at, 0, lines - 1) * 2 + side

    def forward(step):
        block = block_of(step)
        await_rows(slot_x, block)
        core2_copy(block).start()

    ring = partial.shape[0]

    def core_sum_copy(step):
        return remote(
            partial.at[step % ring, pl.ds((1 - core_of) * 2, 2)],
            from_core.at[step],
            s1_sem.at[step],
            r1_sem.at[step],
            group,
            core_peer,
        )

    def x_sum_copy(step):
        return remote(
            partial.at[step % ring, slot_x], from_x.at[step], s2_sem.at[step], r2_sem.at[step], group, x_peer
        )

    def return_copy(step):
        to = block_of(step)
        return remote(
            partial.at[step % ring, mine], returned.at[group], s3_sem.at[to], r3_sem.at[group], to, tp
        )

    def left(step):
        core_sum_copy(step).wait_send()
        x_sum_copy(step).wait_send()

        @pl.when(step < ep_size - 1)
        def _():
            return_copy(step).wait_send()

    def expert_stage(step):
        block = block_of(step)
        await_rows(slot_core, block)
        await_rows(slot_diagonal, block)

        @pl.when(step >= ring)
        def _():
            left(jnp.maximum(step - ring, 0))

        for expert in range(experts_local):
            piece = joined(arrived[:, block, expert])
            gate_proj = dot(piece, gate[expert])
            up_proj = dot(piece, up[expert])
            hidden = (jax.nn.silu(gate_proj) * up_proj).astype(BF16)
            for start in range(0, width, tile):
                part = dot(hidden, down[expert, :, start : start + tile])
                part = part.reshape(4, capacity, tile).astype(BF16)
                partial[step % ring, :, expert, :, start : start + tile] = part
        core_sum_copy(step).start()

    def core_stage(step):
        core_sum_copy(step).wait_recv()
        for slot_of, x_at in ((slot_x, 1 - x_of), (mine, x_of)):
            for expert in range(experts_local):
                total = partial[step % ring, slot_of, expert].astype(F32) + from_core[
                    step, x_at, expert
                ].astype(F32)
                partial[step % ring, slot_of, expert] = total.astype(BF16)
        x_sum_copy(step).start()

    def x_stage(step):
        x_sum_copy(step).wait_recv()
        for expert in range(experts_local):
            total = partial[step % ring, mine, expert].astype(F32) + from_x[step, expert].astype(F32)
            partial[step % ring, mine, expert] = total.astype(BF16)

        @pl.when(step < ep_size - 1)
        def _():
            return_copy(step).start()

    early = (line == lines - 1) & (ring == ep_size)
    late_steps = jnp.where(early, ep_size - 2, ep_size)

    def attend(step, carry):
        @pl.when(step <= chain_of)
        def _():
            await_kv(base + jnp.maximum(place - 2 * step, 0))

            @pl.when(chain_of + 1 < chains)
            def _():
                chain_copy(step).start()

            pair_copy(step).start()

        @pl.when(step == chain_of)
        def _():
            send_up(line)

        @pl.when(line < lines - 1)
        def _():
            exchange(step)

        @pl.when(step <= place)
        def _():
            block = base + jnp.maximum(place - step, 0)

            @pl.when(step % 2 == 1)
            def _():
                await_kv(block)

            def next_visit(head, carry):
                summed, total = visit(block, head, False)
                passed = later[head]
                output[head] = output[head] + jnp.exp(passed) * summed
                later[head] = passed + total
                return carry

            lax.fori_loop(0, heads, next_visit, 0)

        @pl.when(step == 1)
        def _():
            for load in loads:
                load.wait()

        @pl.when(early & (step == 2))
        def _():
            core_stage(ep_size - 1)
            forward(ep_size - 2)
            expert_stage(ep_size - 2)

        @pl.when(early & (step == 3))
        def _():
            core_stage(ep_size - 2)

        @pl.when(line == lines - 1)
        def _():
            exchange(step)

        @pl.when(early & (step == 1))
        def _():
            forward(ep_size - 1)
            expert_stage(ep_size - 1)

        return carry

    lax.fori_loop(1, ep_size, attend, 0)
    last = line - (ep_size - 1) // 2

    forward(0)

    attended = jnp.zeros((rows, heads * DH), F32)
    for head in range(heads):
        attended = attended + lax.dot_general(
            output[head].astype(BF16),
            select[head].astype(BF16),
            (((1,), (1,)), ((), ())),
            preferred_element_type=F32,
        )
    attended = attended.astype(BF16)
    share = projected.shape[1]
    for to in range(projected.shape[0]):
        for start in range(0, width, tile):
            block = dot(attended[to * share : (to + 1) * share], mixer[:, start : start + tile])
            projected[(to % 2) * 2 + to // 2, :, start : start + tile] = block.astype(BF16)

    mixer_core_copy = remote(
        projected.at[pl.ds((1 - core_of) * 2, 2)], mixer_core, mixer_sem.at[0], mixer_sem.at[1], group, core_peer
    )
    mixer_x_copy = remote(
        projected.at[slot_x], mixer_x, mixer_sem.at[2], mixer_sem.at[3], group, x_peer
    )
    mixer_core_copy.start()

    def work(step, carry):
        @pl.when(step < late_steps)
        def _():
            @pl.when((step == 1) & (last >= 0))
            def _():
                cross(jnp.maximum(last, 0))

            @pl.when(step + 1 < late_steps)
            def _():
                forward(step + 1)

            expert_stage(step)

        @pl.when((step >= 1) & (step <= late_steps))
        def _():
            core_stage(step - 1)

        @pl.when(early & (step == 0))
        def _():
            x_stage(ep_size - 2)
            x_stage(ep_size - 1)

        @pl.when(step == ep_size - 1)
        def _():
            mixer_core_copy.wait_recv()
            for slot_of, x_at in ((slot_x, 1 - x_of), (mine, x_of)):
                total = projected[slot_of].astype(F32) + mixer_core[x_at].astype(F32)
                projected[slot_of] = total.astype(BF16)
            mixer_x_copy.start()
            gate_proj = dot(normed[...], shared_gate[...])
            up_proj = dot(normed[...], shared_up[...])
            hidden = (jax.nn.silu(gate_proj) * up_proj).astype(BF16)
            for start in range(0, width, tile):
                shared_out[:, start : start + tile] = dot(hidden, shared_down[:, start : start + tile])

        @pl.when((step >= 2) & (step < late_steps + 2))
        def _():
            x_stage(step - 2)

        return carry

    lax.fori_loop(0, ep_size + 2, work, 0)
    returned[group] = partial[(ep_size - 1) % ring, mine]

    mixer_x_copy.wait_recv()
    total = projected[mine].astype(F32) + mixer_x[...].astype(F32)
    scale = lax.rsqrt(jnp.mean(total * total, axis=-1, keepdims=True) + norm_eps)
    mixer_out_ref[...] = (total * scale * as_row(mixer_gain_ref)).astype(BF16)

    def await_return(step, carry):
        block = (group + 1 + step) % ep_size
        remote(
            returned.at[block], returned.at[block], s3_sem.at[block], r3_sem.at[block], block, tp
        ).wait_recv()
        return carry

    lax.fori_loop(0, ep_size - 1, await_return, 0)
    for start in range(0, width, tile):
        results = joined(returned[:, :, :, start : start + tile])
        mixed = lax.dot_general(
            mixing[...], results, (((0,), (0,)), ((), ())), preferred_element_type=F32
        )
        expert_out_ref[:, start : start + tile] = (
            mixed + shared_out[:, start : start + tile]
        ).astype(BF16)

    @pl.when(chain_of + 1 < chains)
    def _():
        def done(step, carry):
            chain_copy(step).wait_send()
            return carry

        lax.fori_loop(0, chain_of + 1, done, 0)

    @pl.when(pair_of == 0)
    def _():
        pair_copy(0).wait_send()

    def pair_done(step, carry):
        pair_copy(step).wait_send()
        return carry

    lax.fori_loop(1, chain_of + 1, pair_done, 0)

    @pl.when(line + 1 < lines)
    def _():
        def done(at, carry):
            for copy in raw_copies(at, upper, raw_up, info_up):
                copy.wait_send()
            return carry

        lax.fori_loop(0, line + 1, done, 0)

    @pl.when(line > 0)
    def _():
        def done(at, carry):
            for copy in raw_copies(at, lower, raw_down, info_down):
                copy.wait_send()
            return carry

        lax.fori_loop(line, lines, done, 0)

    def crossed(at, carry):
        y_copy(at).wait_send()
        return carry

    lax.fori_loop(0, lines, crossed, 0)

    def forwarded(block, carry):
        x_copy(arrived.at[mine, block], block).wait_send()
        core_copy(arrived.at[mine, block], block).wait_send()
        core2_copy(block).wait_send()
        return carry

    lax.fori_loop(0, ep_size, forwarded, 0)

    def summed_up(step, carry):
        left(step)
        return carry

    lax.fori_loop(ep_size - ring, ep_size, summed_up, 0)
    mixer_core_copy.wait_send()
    mixer_x_copy.wait_send()


def hand_over_kernel(mixer_ref, expert_ref, mixer_out_ref, expert_out_ref):
    mixer_out_ref[...] = mixer_ref[...]
    expert_out_ref[...] = expert_ref[...]


def on_device(
    query_rows,
    key_rows,
    value_rows,
    break_bias,
    mixer_weight,
    mixer_gain,
    expert_input,
    expert_gain,
    route_ids,
    route_weights,
    expert_gate,
    expert_up,
    expert_down,
    shared_gate,
    shared_up,
    shared_down,
):
    rows = query_rows.shape[0]
    heads = query_rows.shape[1] // DH
    kv_width = key_rows.shape[1]
    kv_heads = kv_width // DH
    ep_size = lax.axis_size("ep")
    tp_size = lax.axis_size("tp")
    tokens, width = expert_input.shape
    experts_local, _, hidden = expert_gate.shape
    capacity = 2 * tokens * TOPK // (experts_local * ep_size)
    slots = experts_local * ep_size * capacity
    parts = -(-rows // (2 * kv_width))
    block_rows = rows + 8 * (parts + parts % 2)
    share = rows // tp_size
    lines = ep_size // 2
    cfg = (ep_size, experts_local, capacity, heads, kv_heads)
    piece = (experts_local, capacity, width)
    vmem = pl.BlockSpec(memory_space=pltpu.VMEM)
    hbm = pl.BlockSpec(memory_space=pl.ANY)
    dma = pltpu.SemaphoreType.DMA
    results = pl.pallas_call(
        functools.partial(layer_kernel, cfg),
        out_shape=(
            jax.ShapeDtypeStruct((share, width), BF16),
            jax.ShapeDtypeStruct((tokens, width), BF16),
        ),
        in_specs=[vmem] * 9 + [hbm] * 7,
        out_specs=(vmem, vmem),
        scratch_shapes=[
            pltpu.VMEM((tp_size, ep_size) + piece, BF16),
            pltpu.VMEM((lines, tokens, width), BF16),
            pltpu.VMEM((lines, 8, tokens), F32),
            pltpu.VMEM((lines,) + piece, BF16),
            pltpu.VMEM((min(ep_size, 8), tp_size) + piece, BF16),
            pltpu.VMEM((ep_size, 2) + piece, BF16),
            pltpu.VMEM((ep_size,) + piece, BF16),
            pltpu.VMEM((ep_size,) + piece, BF16),
            pltpu.VMEM(expert_gate.shape, BF16),
            pltpu.VMEM(expert_up.shape, BF16),
            pltpu.VMEM(expert_down.shape, BF16),
            pltpu.VMEM(shared_gate.shape, BF16),
            pltpu.VMEM(shared_up.shape, BF16),
            pltpu.VMEM(shared_down.shape, BF16),
            pltpu.VMEM(mixer_weight.shape, BF16),
            pltpu.VMEM((ep_size, block_rows, 2 * kv_width), BF16),
            pltpu.VMEM((tp_size, share, width), BF16),
            pltpu.VMEM((2, share, width), BF16),
            pltpu.VMEM((share, width), BF16),
            pltpu.VMEM((heads, rows, kv_width), F32),
            pltpu.VMEM((heads, rows, 1), F32),
            pltpu.VMEM((heads, rows, kv_width), BF16),
            pltpu.VMEM((tokens, width), BF16),
            pltpu.VMEM((slots, tokens), BF16),
            pltpu.VMEM((tokens, width), F32),
            dma((7,)),
            dma((ep_size,)),
            dma((ep_size,)),
            dma((ep_size,)),
            dma((tp_size, ep_size)),
            dma((lines,)),
            dma((lines,)),
            dma((lines,)),
            dma((lines,)),
            dma((lines,)),
            dma((lines,)),
            dma((lines,)),

            dma((ep_size,)),
            dma((ep_size,)),
            dma((ep_size,)),
            dma((ep_size,)),
            dma((ep_size,)),
            dma((ep_size,)),
            dma((ep_size,)),
            dma((ep_size,)),
            dma((ep_size,)),
            dma((4,)),
        ],
        compiler_params=pltpu.CompilerParams(
            collective_id=0, has_side_effects=True, vmem_limit_bytes=67043328
        ),
        name="layer",
    )(
        query_rows,
        key_rows,
        value_rows,
        break_bias.T,
        mixer_gain.reshape(-1, 128),
        expert_input,
        expert_gain.reshape(-1, 128),
        route_ids.T,
        route_weights.T,
        mixer_weight,
        expert_gate,
        expert_up,
        expert_down,
        shared_gate,
        shared_up,
        shared_down,
    )
    return pl.pallas_call(
        hand_over_kernel,
        out_shape=tuple(jax.ShapeDtypeStruct(result.shape, BF16) for result in results),
        in_specs=[vmem] * 2,
        out_specs=(vmem, vmem),
        name="hand_over",
    )(*results)


def solution(mesh):
    return jax.shard_map(
        on_device,
        mesh=mesh,
        in_specs=(
            P("ep", "tp"),
            P("ep", "tp"),
            P("ep", "tp"),
            P("ep", "tp"),
            P("tp", None),
            P(),
            P(("ep", "tp"), None),
            P(),
            P("ep", None),
            P(("ep", "tp"), None),
            P("ep", None, "tp"),
            P("ep", None, "tp"),
            P("ep", "tp", None),
            P(),
            P(),
            P(),
        ),
        out_specs=(P(("ep", "tp"), None), P(("ep", "tp"), None)),
        check_vma=False,
    )
```

```python
import functools

import jax
import jax.numpy as jnp
from jax import lax
from jax.experimental import pallas as pl
from jax.experimental.pallas import tpu as pltpu
from jax.sharding import PartitionSpec as P

DH = 64
TOPK = 2
SEQS = 1
MESH = pl.DeviceIdType.MESH

norm_eps = 1e-06
F32 = jnp.float32
BF16 = jnp.bfloat16


def dot(left, right):
    return jnp.dot(left, right, preferred_element_type=F32)


def iota(shape, dim):
    return lax.broadcasted_iota(jnp.int32, shape, dim)


def as_row(ref):
    values = ref[...].astype(F32)
    return jnp.concatenate([values[at : at + 1] for at in range(values.shape[0])], axis=1)


def joined(values):
    rows = values.shape[-2]
    flat = (-1, values.shape[-1])
    if rows % 16:
        return values.astype(F32).reshape(flat).astype(BF16)
    return values.reshape(flat)


def layer_kernel(
    cfg,
    query_ref,
    key_ref,
    value_ref,
    bias_ref,
    mixer_gain_ref,
    input_ref,
    expert_gain_ref,
    ids_ref,
    route_ref,
    mixer_hbm,
    gate_hbm,
    up_hbm,
    down_hbm,
    shared_gate_hbm,
    shared_up_hbm,
    shared_down_hbm,
    mixer_out_ref,
    expert_out_ref,
    arrived,
    raw,
    info,
    crossing,
    partial,
    from_core,
    from_x,
    returned,
    gate,
    up,
    down,
    shared_gate,
    shared_up,
    shared_down,
    mixer,
    kv,
    projected,
    mixer_core,
    mixer_x,
    output,
    later,
    queries,
    normed,
    mixing,
    shared_out,
    weight_sem,
    kv_recv,
    kv_chain,
    kv_pair,
    arrive_sem,
    raw_recv,
    raw_up,
    raw_down,
    info_recv,
    info_up,
    info_down,
    y_sem,
    x_sem,
    core_sem,
    core2_sem,
    s1_sem,
    r1_sem,
    s2_sem,
    r2_sem,
    s3_sem,
    r3_sem,
    mixer_sem,
):
    ep_size, experts_local, capacity, heads, kv_heads = cfg
    group = lax.axis_index("ep").astype(jnp.int32)
    tp = lax.axis_index("tp").astype(jnp.int32)
    rows, kv_width = key_ref.shape
    tokens, width = input_ref.shape
    experts = experts_local * ep_size
    groups = heads // kv_heads
    span = ep_size // SEQS

    core_of, x_of = tp % 2, tp // 2
    core_peer = tp + 1 - 2 * core_of
    x_peer = x_of * -2 + core_of + 2
    mine = core_of * 2 + x_of
    slot_core = (1 - core_of) * 2 + x_of
    slot_x = core_of * 2 + 1 - x_of
    slot_diagonal = (1 - core_of) * 2 + 1 - x_of

    place = group % span
    base = group - place
    pair_of, chain_of = place % 2, place // 2
    pair = group + 1 - 2 * pair_of
    chains = span // 2
    above = jnp.where(chain_of + 1 < chains, group + 2, group)
    line, lines = group // 2, ep_size // 2
    upper = jnp.where(line + 1 < lines, group + 2, group)
    lower = jnp.where(line > 0, group - 2, group)

    def remote(source, target, sent, received, ep, to):
        return pltpu.make_async_remote_copy(
            src_ref=source,
            dst_ref=target,
            send_sem=sent,
            recv_sem=received,
            device_id=(ep, to),
            device_id_type=MESH,
        )

    barrier = pltpu.get_barrier_semaphore()

    def greet(step, carry):
        other = (group + 1 + step) % ep_size
        pl.semaphore_signal(barrier, inc=1, device_id=(other, tp), device_id_type=MESH)
        return carry

    lax.fori_loop(0, ep_size - 1, greet, 0)
    for to in (core_peer, x_peer):
        pl.semaphore_signal(barrier, inc=1, device_id=(group, to), device_id_type=MESH)

    loads = []
    for source, target in (
        (mixer_hbm, mixer),
        (gate_hbm, gate),
        (up_hbm, up),
        (down_hbm, down),
        (shared_gate_hbm, shared_gate),
        (shared_up_hbm, shared_up),
        (shared_down_hbm, shared_down),
    ):
        load = pltpu.make_async_copy(source, target, weight_sem.at[len(loads)])
        load.start()
        loads.append(load)

    parts = -(-rows // (2 * kv_width))
    kv[group, 0:rows, 0:kv_width] = key_ref[...]
    kv[group, 0:rows, kv_width : 2 * kv_width] = value_ref[...]
    biases = jnp.concatenate([bias_ref[...].astype(F32), jnp.zeros((8 - heads, rows), F32)], axis=0)
    pieces = []
    for part in range(parts):
        piece = biases[:, part * 2 * kv_width : min(rows, (part + 1) * 2 * kv_width)]
        missing = 2 * kv_width - piece.shape[1]
        if missing:
            piece = jnp.concatenate([piece, jnp.zeros((8, missing), F32)], axis=1)
        pieces.append(piece)
    while len(pieces) % 2:
        pieces.append(jnp.zeros((8, 2 * kv_width), F32))
    kv[group, rows : rows + 8 * len(pieces), :] = jnp.concatenate(pieces, axis=0).astype(BF16)

    first_token = pl.multiple_of(tp * tokens, tokens)
    first_id = ids_ref[0:1, pl.ds(first_token, tokens)]
    second_id = ids_ref[1:2, pl.ds(first_token, tokens)]
    number = iota((experts, tokens), 0)
    is_first, is_second = number == first_id, number == second_id
    named = jnp.where(is_first | is_second, 1.0, 0.0).astype(BF16)
    weight = jnp.where(is_first, route_ref[0:1, :], jnp.where(is_second, route_ref[1:2, :], 0.0))
    earlier = (iota((tokens, tokens), 0) < iota((tokens, tokens), 1)).astype(F32).astype(BF16)
    before = dot(named, earlier)
    info[line] = jnp.concatenate(
        [
            first_id.astype(F32),
            jnp.sum(jnp.where(is_first, before, 0.0), axis=0, keepdims=True),
            second_id.astype(F32),
            jnp.sum(jnp.where(is_second, before, 0.0), axis=0, keepdims=True),
            jnp.zeros((4, tokens), F32),
        ],
        axis=0,
    )
    values = input_ref[...].astype(F32)
    scale = lax.rsqrt(jnp.mean(values * values, axis=-1, keepdims=True) + norm_eps)
    values = (values * scale * as_row(expert_gain_ref)).astype(BF16)
    normed[...] = values
    raw[line] = values
    tile = min(width, 512)

    half = experts_local * capacity
    row = iota((2 * half, tokens), 0)
    own_half = row < half
    row_expert = jnp.where(own_half, row // capacity + group * experts_local, row // capacity + (pair - 1) * experts_local)
    row_expert = row_expert.astype(F32)
    row_rank = (row % capacity).astype(F32)

    def pick(at):
        told = info[at]
        wanted = ((row_expert == told[0:1]) & (row_rank == told[1:2])) | (
            (row_expert == told[2:3]) & (row_rank == told[3:4])
        )
        wanted = jnp.where(wanted, 1.0, 0.0).astype(BF16)
        for start in range(0, width, tile):
            block = dot(wanted, raw[at, :, start : start + tile])
            block = block.reshape(2, experts_local, capacity, tile).astype(BF16)
            arrived[mine, 2 * at + pair_of, :, :, start : start + tile] = block[0]
            crossing[at, :, :, start : start + tile] = block[1]

    pick(line)

    select = {}
    for head in range(heads):
        shape = (heads * DH, kv_width)
        inside = iota(shape, 1) - (head // groups) * DH
        picked = (iota(shape, 0) - head * DH == inside) & (inside >= 0) & (inside < DH)
        select[head] = picked.astype(F32)
        queries[head] = dot(query_ref[...], (select[head] * DH ** (-0.5)).astype(BF16)).astype(BF16)

    slots = experts * capacity
    slot = iota((slots, experts), 0)
    owner = iota((slots, experts), 1) * capacity
    spread = ((slot >= owner) & (slot < owner + capacity)).astype(F32).astype(BF16)
    rank = (iota((slots, tokens), 0) % capacity).astype(F32)
    chosen = (dot(spread, named) > 0.5) & (dot(spread, before.astype(BF16)) == rank)
    mixing[...] = jnp.where(chosen, dot(spread, weight.astype(BF16)), 0.0).astype(BF16)

    pl.semaphore_wait(barrier, ep_size + 1)

    def chain_copy(step):
        block = base + jnp.maximum(place - 2 * step, 0)
        return remote(kv.at[block], kv.at[block], kv_chain.at[step], kv_recv.at[block], above, tp)

    def pair_copy(step):
        block = base + jnp.maximum(place - 2 * step, 0)
        return remote(kv.at[block], kv.at[block], kv_pair.at[step], kv_recv.at[block], pair, tp)

    def await_kv(block):
        remote(kv.at[block], kv.at[block], kv_chain.at[0], kv_recv.at[block], pair, tp).wait_recv()

    @pl.when(chain_of + 1 < chains)
    def _():
        chain_copy(0).start()

    @pl.when(pair_of == 0)
    def _():
        pair_copy(0).start()

    def raw_copies(at, to, raw_sent, info_sent):
        return (
            remote(raw.at[at], raw.at[at], raw_sent.at[at], raw_recv.at[at], to, tp),
            remote(info.at[at], info.at[at], info_sent.at[at], info_recv.at[at], to, tp),
        )

    def send_up(at):
        @pl.when(line + 1 < lines)
        def _():
            for copy in raw_copies(at, upper, raw_up, info_up):
                copy.start()

    def send_down(at):
        @pl.when(line > 0)
        def _():
            for copy in raw_copies(at, lower, raw_down, info_down):
                copy.start()

    def y_copy(at):
        block = 2 * at + pair_of
        return remote(crossing.at[at], arrived.at[mine, block], y_sem.at[at], arrive_sem.at[mine, block], pair, tp)

    def x_copy(source, block):
        return remote(source, arrived.at[mine, block], x_sem.at[block], arrive_sem.at[mine, block], group, x_peer)

    def core_copy(source, block):
        return remote(
            source, arrived.at[mine, block], core_sem.at[block], arrive_sem.at[mine, block], group, core_peer
        )

    def core2_copy(block):
        part = arrived.at[slot_x, block]
        return remote(part, part, core2_sem.at[block], arrive_sem.at[slot_x, block], group, core_peer)

    def await_rows(place_of, block):
        part = arrived.at[place_of, block]
        remote(part, part, core_sem.at[block], arrive_sem.at[place_of, block], group, x_peer).wait_recv()

    def pass_on(block):
        x_copy(arrived.at[mine, block], block).start()
        core_copy(arrived.at[mine, block], block).start()

    def cross(at):
        block = 2 * at + 1 - pair_of
        await_rows(mine, block)
        pass_on(block)

    def take(at):
        pick(at)
        pass_on(2 * at + pair_of)
        y_copy(at).start()

    pass_on(group)
    y_copy(line).start()
    send_down(line)

    @pl.when(chain_of == 0)
    def _():
        send_up(line)

    row_of = iota((rows, rows), 0)
    column_of = iota((rows, rows), 1)
    after = (column_of < row_of).astype(F32).astype(BF16)

    def visit(block, head, diagonal):
        keys = kv[block, 0:rows, 0:kv_width]
        scores = lax.dot_general(
            queries[head], keys, (((1,), (1,)), ((), ())), preferred_element_type=F32
        )
        tail = kv[block, rows : rows + 8 * len(pieces), :].astype(F32)
        bias = []
        for part in range(parts):
            line = jnp.where(iota(tail.shape, 0) == head + 8 * part, tail, 0.0)
            line = jnp.sum(line, axis=0, keepdims=True)
            bias.append(line[:, : min(2 * kv_width, rows - part * 2 * kv_width)])
        scores = scores + jnp.concatenate(bias, axis=1)
        soft = jnp.log(1.0 + jnp.exp(-jnp.abs(scores)))
        keep = -(jnp.maximum(scores, 0.0) + soft)
        if diagonal:
            keep = jnp.where(column_of < row_of, keep, 0.0)
        high = keep.astype(BF16)
        low = (keep - high.astype(F32)).astype(BF16)
        beyond = dot(high, after) + dot(low, after)
        weights = jnp.exp(jnp.minimum(scores, 0.0) - soft + beyond)
        if diagonal:
            weights = jnp.where(column_of < row_of, weights, 0.0)
        total = beyond[:, 0:1] + keep[:, 0:1]
        summed = dot(weights.astype(BF16), kv[block, 0:rows, kv_width : 2 * kv_width])
        return summed, total

    def first_visit(head, carry):
        summed, total = visit(group, head, True)
        output[head] = summed
        later[head] = total
        return carry

    lax.fori_loop(0, heads, first_visit, 0)

    def cross_before(step):
        @pl.when(step == 1)
        def _():
            cross(line)

        @pl.when(step > 2)
        def _():
            at = jnp.where(step % 2 == 1, line + step // 2, line - (step - 2) // 2)

            @pl.when((at >= 0) & (at < lines))
            def _():
                cross(jnp.clip(at, 0, lines - 1))

    def take_next(step):
        @pl.when(step > 1)
        def _():
            at = jnp.where(step % 2 == 0, line + step // 2, line - step // 2)
            at_in = jnp.clip(at, 0, lines - 1)

            @pl.when((at >= 0) & (at < lines))
            def _():
                for copy in raw_copies(at_in, upper, raw_up, info_up):
                    copy.wait_recv()

            @pl.when((at > line) & (at < lines))
            def _():
                send_down(at_in)

            @pl.when((at >= 0) & (at < line))
            def _():
                send_up(at_in)

            @pl.when((at >= 0) & (at < lines))
            def _():
                take(at_in)

    roomy = partial.shape[0] == ep_size
    is_last = (line == lines - 1) & roomy
    is_first_line = (line == 0) & roomy
    early = is_last | is_first_line
    own_step = jnp.where(is_first_line, ep_size - 2, ep_size - 1)
    late_steps = jnp.where(is_last, ep_size - 2, jnp.where(is_first_line, ep_size - 1, ep_size))

    def block_of(step):
        index = step // 2
        middle = lines // 2
        lower_half = line < middle
        depth = jnp.where(lower_half, middle - line, line - middle + 1)
        turned = (index + depth) % middle
        across = jnp.where(lower_half, middle + turned, middle - 1 - turned)
        start = jnp.where(lower_half, 0, middle)
        beside = start + (line - start + 1 + index) % middle
        at = jnp.where(index < middle, across, beside)
        at = jnp.where(index < lines - 1, at, line)
        last_side = jnp.where(step == own_step, pair_of, 1 - pair_of)
        side = jnp.where(index < lines - 1, (pair_of + step) % 2, last_side)
        return jnp.clip(at, 0, lines - 1) * 2 + side

    def forward(step):
        block = block_of(step)
        await_rows(slot_x, block)
        core2_copy(block).start()

    ring = partial.shape[0]

    def core_sum_copy(step):
        return remote(
            partial.at[step % ring, pl.ds((1 - core_of) * 2, 2)],
            from_core.at[step],
            s1_sem.at[step],
            r1_sem.at[step],
            group,
            core_peer,
        )

    def x_sum_copy(step):
        return remote(
            partial.at[step % ring, slot_x], from_x.at[step], s2_sem.at[step], r2_sem.at[step], group, x_peer
        )

    def return_copy(step):
        to = block_of(step)
        return remote(
            partial.at[step % ring, mine], returned.at[group], s3_sem.at[to], r3_sem.at[group], to, tp
        )

    def left(step):
        core_sum_copy(step).wait_send()
        x_sum_copy(step).wait_send()

        @pl.when(step != own_step)
        def _():
            return_copy(step).wait_send()

    def expert_stage(step):
        block = block_of(step)
        await_rows(slot_core, block)
        await_rows(slot_diagonal, block)

        @pl.when(step >= ring)
        def _():
            left(jnp.maximum(step - ring, 0))

        for expert in range(experts_local):
            piece = joined(arrived[:, block, expert])
            gate_proj = dot(piece, gate[expert])
            up_proj = dot(piece, up[expert])
            hidden = (jax.nn.silu(gate_proj) * up_proj).astype(BF16)
            for start in range(0, width, tile):
                part = dot(hidden, down[expert, :, start : start + tile])
                part = part.reshape(4, capacity, tile).astype(BF16)
                partial[step % ring, :, expert, :, start : start + tile] = part
        core_sum_copy(step).start()

    def core_stage(step):
        core_sum_copy(step).wait_recv()
        for slot_of, x_at in ((slot_x, 1 - x_of), (mine, x_of)):
            for expert in range(experts_local):
                total = partial[step % ring, slot_of, expert].astype(F32) + from_core[
                    step, x_at, expert
                ].astype(F32)
                partial[step % ring, slot_of, expert] = total.astype(BF16)
        x_sum_copy(step).start()

    def x_stage(step):
        x_sum_copy(step).wait_recv()
        for expert in range(experts_local):
            total = partial[step % ring, mine, expert].astype(F32) + from_x[step, expert].astype(F32)
            partial[step % ring, mine, expert] = total.astype(BF16)

        @pl.when(step != own_step)
        def _():
            return_copy(step).start()

    def early_step(step):
        return jnp.where(is_last & (step == 2), ep_size - 2, ep_size - 1)

    def attend(step, carry):
        @pl.when((is_last & (step == 2)) | (early & (step == 3)))
        def _():
            core_stage(early_step(step - 1))

        @pl.when(step <= chain_of)
        def _():
            await_kv(base + jnp.maximum(place - 2 * step, 0))

            @pl.when(chain_of + 1 < chains)
            def _():
                chain_copy(step).start()

            pair_copy(step).start()

        @pl.when(step == chain_of)
        def _():
            send_up(line)

        @pl.when(line == lines // 2)
        def _():
            take_next(step)
            cross_before(step)

        @pl.when((line < lines - 1) & (line != lines // 2))
        def _():
            cross_before(step)
            take_next(step)

        @pl.when(step <= place)
        def _():
            block = base + jnp.maximum(place - step, 0)

            @pl.when(step % 2 == 1)
            def _():
                await_kv(block)

            def next_visit(head, carry):
                summed, total = visit(block, head, False)
                passed = later[head]
                output[head] = output[head] + jnp.exp(passed) * summed
                later[head] = passed + total
                return carry

            lax.fori_loop(0, heads, next_visit, 0)

        @pl.when(step == 1)
        def _():
            for load in loads:
                load.wait()

        @pl.when(line == lines - 1)
        def _():
            cross_before(step)
            take_next(step)

        @pl.when((is_last & (step == 1)) | (early & (step == 2)))
        def _():
            soon = early_step(step)
            forward(soon)
            expert_stage(soon)

        return carry

    lax.fori_loop(1, ep_size, attend, 0)
    last = line - (ep_size - 1) // 2

    forward(0)

    attended = jnp.zeros((rows, heads * DH), F32)
    for head in range(heads):
        attended = attended + lax.dot_general(
            output[head].astype(BF16),
            select[head].astype(BF16),
            (((1,), (1,)), ((), ())),
            preferred_element_type=F32,
        )
    attended = attended.astype(BF16)
    share = projected.shape[1]
    for to in range(projected.shape[0]):
        for start in range(0, width, tile):
            block = dot(attended[to * share : (to + 1) * share], mixer[:, start : start + tile])
            projected[(to % 2) * 2 + to // 2, :, start : start + tile] = block.astype(BF16)

    mixer_core_copy = remote(
        projected.at[pl.ds((1 - core_of) * 2, 2)], mixer_core, mixer_sem.at[0], mixer_sem.at[1], group, core_peer
    )
    mixer_x_copy = remote(
        projected.at[slot_x], mixer_x, mixer_sem.at[2], mixer_sem.at[3], group, x_peer
    )
    mixer_core_copy.start()

    def work(step, carry):
        @pl.when(step < late_steps)
        def _():
            @pl.when((step == 1) & (last >= 0))
            def _():
                cross(jnp.maximum(last, 0))

            @pl.when(step + 1 < late_steps)
            def _():
                forward(step + 1)

            expert_stage(step)

        @pl.when((step >= 1) & (step <= late_steps))
        def _():
            core_stage(step - 1)

        @pl.when((is_last & (step == 0)) | (early & (step == 1)))
        def _():
            x_stage(jnp.where(is_last & (step == 0), ep_size - 2, ep_size - 1))

        @pl.when(step == ep_size - 1)
        def _():
            mixer_core_copy.wait_recv()
            for slot_of, x_at in ((slot_x, 1 - x_of), (mine, x_of)):
                total = projected[slot_of].astype(F32) + mixer_core[x_at].astype(F32)
                projected[slot_of] = total.astype(BF16)
            mixer_x_copy.start()
            gate_proj = dot(normed[...], shared_gate[...])
            up_proj = dot(normed[...], shared_up[...])
            hidden = (jax.nn.silu(gate_proj) * up_proj).astype(BF16)
            for start in range(0, width, tile):
                shared_out[:, start : start + tile] = dot(hidden, shared_down[:, start : start + tile])

        @pl.when((step >= 2) & (step < late_steps + 2))
        def _():
            x_stage(step - 2)

        return carry

    lax.fori_loop(0, ep_size + 2, work, 0)
    returned[group] = partial[own_step % ring, mine]

    mixer_x_copy.wait_recv()
    total = projected[mine].astype(F32) + mixer_x[...].astype(F32)
    scale = lax.rsqrt(jnp.mean(total * total, axis=-1, keepdims=True) + norm_eps)
    mixer_out_ref[...] = (total * scale * as_row(mixer_gain_ref)).astype(BF16)

    def await_return(step, carry):
        block = (group + 1 + step) % ep_size
        remote(
            returned.at[block], returned.at[block], s3_sem.at[block], r3_sem.at[block], block, tp
        ).wait_recv()
        return carry

    lax.fori_loop(0, ep_size - 1, await_return, 0)
    for start in range(0, width, tile):
        results = joined(returned[:, :, :, start : start + tile])
        mixed = lax.dot_general(
            mixing[...], results, (((0,), (0,)), ((), ())), preferred_element_type=F32
        )
        expert_out_ref[:, start : start + tile] = (
            mixed + shared_out[:, start : start + tile]
        ).astype(BF16)

    @pl.when(chain_of + 1 < chains)
    def _():
        def done(step, carry):
            chain_copy(step).wait_send()
            return carry

        lax.fori_loop(0, chain_of + 1, done, 0)

    @pl.when(pair_of == 0)
    def _():
        pair_copy(0).wait_send()

    def pair_done(step, carry):
        pair_copy(step).wait_send()
        return carry

    lax.fori_loop(1, chain_of + 1, pair_done, 0)

    @pl.when(line + 1 < lines)
    def _():
        def done(at, carry):
            for copy in raw_copies(at, upper, raw_up, info_up):
                copy.wait_send()
            return carry

        lax.fori_loop(0, line + 1, done, 0)

    @pl.when(line > 0)
    def _():
        def done(at, carry):
            for copy in raw_copies(at, lower, raw_down, info_down):
                copy.wait_send()
            return carry

        lax.fori_loop(line, lines, done, 0)

    def crossed(at, carry):
        y_copy(at).wait_send()
        return carry

    lax.fori_loop(0, lines, crossed, 0)

    def forwarded(block, carry):
        x_copy(arrived.at[mine, block], block).wait_send()
        core_copy(arrived.at[mine, block], block).wait_send()
        core2_copy(block).wait_send()
        return carry

    lax.fori_loop(0, ep_size, forwarded, 0)

    def summed_up(step, carry):
        left(step)
        return carry

    lax.fori_loop(ep_size - ring, ep_size, summed_up, 0)
    mixer_core_copy.wait_send()
    mixer_x_copy.wait_send()


def hand_over_kernel(mixer_ref, expert_ref, mixer_out_ref, expert_out_ref):
    mixer_out_ref[...] = mixer_ref[...]
    expert_out_ref[...] = expert_ref[...]


def on_device(
    query_rows,
    key_rows,
    value_rows,
    break_bias,
    mixer_weight,
    mixer_gain,
    expert_input,
    expert_gain,
    route_ids,
    route_weights,
    expert_gate,
    expert_up,
    expert_down,
    shared_gate,
    shared_up,
    shared_down,
):
    rows = query_rows.shape[0]
    heads = query_rows.shape[1] // DH
    kv_width = key_rows.shape[1]
    kv_heads = kv_width // DH
    ep_size = lax.axis_size("ep")
    tp_size = lax.axis_size("tp")
    tokens, width = expert_input.shape
    experts_local, _, hidden = expert_gate.shape
    capacity = 2 * tokens * TOPK // (experts_local * ep_size)
    slots = experts_local * ep_size * capacity
    parts = -(-rows // (2 * kv_width))
    block_rows = rows + 8 * (parts + parts % 2)
    share = rows // tp_size
    lines = ep_size // 2
    cfg = (ep_size, experts_local, capacity, heads, kv_heads)
    piece = (experts_local, capacity, width)
    vmem = pl.BlockSpec(memory_space=pltpu.VMEM)
    hbm = pl.BlockSpec(memory_space=pl.ANY)
    dma = pltpu.SemaphoreType.DMA
    results = pl.pallas_call(
        functools.partial(layer_kernel, cfg),
        out_shape=(
            jax.ShapeDtypeStruct((share, width), BF16),
            jax.ShapeDtypeStruct((tokens, width), BF16),
        ),
        in_specs=[vmem] * 9 + [hbm] * 7,
        out_specs=(vmem, vmem),
        scratch_shapes=[
            pltpu.VMEM((tp_size, ep_size) + piece, BF16),
            pltpu.VMEM((lines, tokens, width), BF16),
            pltpu.VMEM((lines, 8, tokens), F32),
            pltpu.VMEM((lines,) + piece, BF16),
            pltpu.VMEM((min(ep_size, 8), tp_size) + piece, BF16),
            pltpu.VMEM((ep_size, 2) + piece, BF16),
            pltpu.VMEM((ep_size,) + piece, BF16),
            pltpu.VMEM((ep_size,) + piece, BF16),
            pltpu.VMEM(expert_gate.shape, BF16),
            pltpu.VMEM(expert_up.shape, BF16),
            pltpu.VMEM(expert_down.shape, BF16),
            pltpu.VMEM(shared_gate.shape, BF16),
            pltpu.VMEM(shared_up.shape, BF16),
            pltpu.VMEM(shared_down.shape, BF16),
            pltpu.VMEM(mixer_weight.shape, BF16),
            pltpu.VMEM((ep_size, block_rows, 2 * kv_width), BF16),
            pltpu.VMEM((tp_size, share, width), BF16),
            pltpu.VMEM((2, share, width), BF16),
            pltpu.VMEM((share, width), BF16),
            pltpu.VMEM((heads, rows, kv_width), F32),
            pltpu.VMEM((heads, rows, 1), F32),
            pltpu.VMEM((heads, rows, kv_width), BF16),
            pltpu.VMEM((tokens, width), BF16),
            pltpu.VMEM((slots, tokens), BF16),
            pltpu.VMEM((tokens, width), F32),
            dma((7,)),
            dma((ep_size,)),
            dma((ep_size,)),
            dma((ep_size,)),
            dma((tp_size, ep_size)),
            dma((lines,)),
            dma((lines,)),
            dma((lines,)),
            dma((lines,)),
            dma((lines,)),
            dma((lines,)),
            dma((lines,)),

            dma((ep_size,)),
            dma((ep_size,)),
            dma((ep_size,)),
            dma((ep_size,)),
            dma((ep_size,)),
            dma((ep_size,)),
            dma((ep_size,)),
            dma((ep_size,)),
            dma((ep_size,)),
            dma((4,)),
        ],
        compiler_params=pltpu.CompilerParams(
            collective_id=0, has_side_effects=True, vmem_limit_bytes=67043328
        ),
        name="layer",
    )(
        query_rows,
        key_rows,
        value_rows,
        break_bias.T,
        mixer_gain.reshape(-1, 128),
        expert_input,
        expert_gain.reshape(-1, 128),
        route_ids.T,
        route_weights.T,
        mixer_weight,
        expert_gate,
        expert_up,
        expert_down,
        shared_gate,
        shared_up,
        shared_down,
    )
    return pl.pallas_call(
        hand_over_kernel,
        out_shape=tuple(jax.ShapeDtypeStruct(result.shape, BF16) for result in results),
        in_specs=[vmem] * 2,
        out_specs=(vmem, vmem),
        name="hand_over",
    )(*results)


def solution(mesh):
    return jax.shard_map(
        on_device,
        mesh=mesh,
        in_specs=(
            P("ep", "tp"),
            P("ep", "tp"),
            P("ep", "tp"),
            P("ep", "tp"),
            P("tp", None),
            P(),
            P(("ep", "tp"), None),
            P(),
            P("ep", None),
            P(("ep", "tp"), None),
            P("ep", None, "tp"),
            P("ep", None, "tp"),
            P("ep", "tp", None),
            P(),
            P(),
            P(),
        ),
        out_specs=(P(("ep", "tp"), None), P(("ep", "tp"), None)),
        check_vma=False,
    )
```
